32 devices in a mesh: sp: 16 (over z, y, x), tp: 2 (over core).
Axes of the slice: x: 2, y: 2, z: 4, core: 2. Of those that a mesh axis runs over, the one named last changes fastest.
Arguments:
- moe_input: bfloat16 [2048, 2048], P('sp'), may hold values from -6 to 6
- out_grad: bfloat16 [2048, 2048], P('sp'), may hold values from -8 to 8
- route_ids: int32 [2048, 2], P('sp'), may hold values from 0 to 7, all different within a row; in each aligned block of 128 rows (0 to 127, 128 to 255, ...) at most 48 rows name the same one
- route_weights: float32 [2048, 2], P('sp'), may hold values from 0.1 to 0.9
- gate_w: bfloat16 [16, 2048, 1792], P('sp', None, 'tp'), may hold values from -0.125 to 0.125
- up_w: bfloat16 [16, 2048, 1792], P('sp', None, 'tp'), may hold values from -0.125 to 0.125
- down_w: bfloat16 [16, 1792, 2048], P('sp', 'tp'), may hold values from -0.09375 to 0.09375
- mixer_out: bfloat16 [2048, 1024], P('sp', 'tp'), may hold values from -6 to 6
- out_weight: bfloat16 [1024, 2048], P('tp'), may hold values from -0.1875 to 0.1875
- queries: bfloat16 [2048, 512], P('sp', 'tp'), may hold values from -0.125 to 0.125
- keys: bfloat16 [2048, 512], P('sp', 'tp'), may hold values from -0.3125 to 0.3125
- values: bfloat16 [2048, 1024], P('sp', 'tp'), may hold values from -1.5 to 1.5
- log_decay: float32 [2048, 512], P('sp', 'tp'), may hold values from -0.1 to 0, as said below
- block_states: float32 [32, 8, 64, 128], P('sp', 'tp'), may hold values from -1.75 to 1.75
Outputs:
- grad_queries: bfloat16 [2048, 512], P('sp', 'tp')
- grad_keys: bfloat16 [2048, 512], P('sp', 'tp')
- grad_values: bfloat16 [2048, 1024], P('sp', 'tp')
- grad_decay: float32 [2048, 512], P('sp', 'tp')
- grad_out_weight: float32 [1024, 2048], P('tp', 'sp')
- grad_gate_w: bfloat16 [16, 2048, 1792], P('sp', None, 'tp')
- grad_up_w: bfloat16 [16, 2048, 1792], P('sp', None, 'tp')
- grad_down_w: bfloat16 [16, 1792, 2048], P('sp', 'tp')
The draws below stay inside these ranges and needn't reach their ends.
Inputs may be any that keep to these rules, and one draw needn't show every extreme that they name: `route_ids`: each row names two different experts. In the rows of one index of sp no expert is named more than 48 times, and in every draw some expert is named exactly 48 times by the rows of some index of sp. `log_decay`: Negative.
All inputs are finite; a program needn't handle non-finite values.
Results may differ from the reference program's by a relative error of at most 0.013.
Values may be sent and summed in bfloat16 or wider, within the bound.
A program may use at most 128 MiB of HBM per device.

```python
import math
import jax
import jax.numpy as jnp
import numpy as np
from jax import lax

D = 2048
HEADS = 8
DK = 64
DV = 128
FFE = 3584
BLK = 64
TOK_DEV = 128
TOKENS = 2048
HK = 512
HV = 1024
NBLK = 32
EXPERTS = 8
FH = 1792
FQ = 896
CAP = 48
SLOTS = 768
N_SP = 16
N_TP = 2


def draw_log_decay(key, part):
    key_kind, key_block, key_rough = jax.random.split(key, 3)
    channels = HEADS * DK
    slow_share = 5
    slow_channel = jax.random.randint(key_kind, (channels,), 0, 10) < slow_share
    base_rate = jnp.where(slow_channel, 2.0 / TOKENS, 1.0 / 40.0).astype(jnp.float32)
    factor = jnp.exp(jax.random.uniform(key_block, (TOKENS // TOK_DEV,), jnp.float32, jnp.log(0.4), jnp.log(2.5)))
    roughness = jax.random.uniform(key_rough, (TOKENS, channels), jnp.float32, 0.5, 1.5)
    per_token = jnp.repeat(factor, TOK_DEV)
    return (-(base_rate[None, :] * per_token[:, None] * roughness)).astype(jnp.float32)


def with_spikes(entries, rng, source, target, shards_of, factor):
    def block_of(axis_at):
        return (jnp.arange(entries.shape[axis_at]) // (entries.shape[axis_at] // shards_of)).reshape((-1,) + (1,) * (entries.ndim - 1 - axis_at))

    first = jax.random.permutation(rng, shards_of)[block_of(target)]
    far = (block_of(target) + shards_of // 2) % shards_of
    return jnp.where((block_of(source) == first) | (block_of(source) == far), factor * entries, entries)


def block_levels(stream_key, dims, cuts, low, top_value):
    factor_of, own = 1.0, jax.random.fold_in(stream_key, 6)
    for dim, shards_of in cuts:
        draws = jnp.exp(jax.random.uniform(jax.random.fold_in(own, dim), (shards_of,), jnp.float32, low / len(cuts), top_value / len(cuts)))
        factor_of = factor_of * jnp.repeat(draws, dims[dim] // shards_of).reshape([-1 if axis == dim else 1 for axis in range(len(dims))])
    return factor_of


def deal_out(own_key, own, number, rows, number_of, top, bound, lean):
    sequence = jax.random.permutation(own_key, number_of)
    packed, common = portions_of(number_of, rows * top, bound, lean, True), portions_of(number_of, rows * top, bound, lean, False)
    places = jnp.arange(number_of)

    def named(lengths, rotation):
        used = int((lengths > 0).sum())
        fixed = max(1, used // 4)
        passed = fixed + (places - fixed + rotation * (used - fixed)) % max(1, number_of - fixed)
        return jnp.zeros((number_of,), jnp.int32).at[sequence[jnp.where(places < fixed, places, passed)]].set(jnp.asarray(lengths, jnp.int32))

    lengths = jnp.where(number % 4 == 0, named(packed, number // 4), named(common, number - number // 4 - 1))
    mixed = jax.random.permutation(jax.random.fold_in(own, 3), number_of)
    donor, taker = mixed[0:number_of // 2 * 2:2], mixed[1:number_of // 2 * 2:2]
    margin = jnp.minimum(lengths[donor] - 1, bound - lengths[taker]) // 2
    margin = jnp.where((donor == sequence[0]) | (taker == sequence[0]) | (lengths[taker] == 0), 0, jnp.maximum(margin, 0))
    passed = jax.random.randint(jax.random.fold_in(own, 4), (number_of // 2,), 0, 1 << 20) % (margin + 1)
    lengths = lengths.at[donor].add(-passed).at[taker].add(passed)
    items = jnp.searchsorted(jnp.cumsum(lengths), jnp.arange(rows * top), side="right").astype(jnp.int32)
    table = items.reshape(top, rows).T
    table = table[jax.random.permutation(jax.random.fold_in(own, 1), rows)]
    rotation = jax.random.randint(jax.random.fold_in(own, 2), (rows, 1), 0, top)
    return jnp.take_along_axis(table, (jnp.arange(top)[None, :] + rotation) % top, axis=1)


def portions_of(count, total, bound, lean, full):
    weights = [(1 << 20) // math.isqrt(rank ** lean) + 1 for rank in range(1, count + 1)]
    largest = bound if full else min(bound, max(-(-total // count), total * weights[0] // sum(weights)))
    least = 1 if total - largest >= count - 1 else 0
    counts, rest = [largest] + [least] * (count - 1), total - largest - least * (count - 1)
    while rest > 0:
        candidates = [i for i in range(1, count) if counts[i] < largest] or [i for i in range(1, count) if counts[i] < bound]
        pool, remaining = sum([weights[i] for i in candidates]), rest
        for i in candidates:
            more = min(bound - counts[i], max(1, remaining * weights[i] // pool), rest)
            counts[i] = counts[i] + more
            rest = rest - more
    return np.array(counts)


def scatter_about(stream_key, shape, deviation, most, shards=(), kind=jnp.bfloat16):
    factor_of = block_levels(stream_key, shape, shards, -0.22, 0.18) if shards else 1.0
    drawn = jax.random.normal(stream_key, shape, jnp.float32) * deviation * factor_of
    return jnp.minimum(jnp.maximum(drawn, -most), most).astype(kind)


def gaussian_with(stream_key, shape, deviation, bound, shards, heavy, kind=jnp.bfloat16):
    entries = deviation * jax.random.normal(stream_key, shape, jnp.float32)
    if shards:
        entries = entries * block_levels(stream_key, shape, shards, -0.22, 0.18)
    return jnp.clip(with_spikes(entries, jax.random.fold_in(stream_key, 3), *heavy), -bound, bound).astype(kind)


def setup_inputs(seed: int = 0) -> dict:
    arg_keys = jax.random.split(jax.random.key(seed), 15)
    moe_input = scatter_about(arg_keys[0], (TOKENS, D), 1.0, 6.0, ((0, 16),))
    out_grad = gaussian_with(arg_keys[1], (TOKENS, D), 1.0, 8.0, ((0, 16),), (0, 1, 16, 2.0))
    route_ids_keys = jax.random.split(jax.random.fold_in(arg_keys[2], 1), TOKENS // TOK_DEV)
    route_ids_turns = jax.random.permutation(jax.random.fold_in(arg_keys[2], 3), TOKENS // TOK_DEV)
    route_ids = jax.vmap(lambda own, number: deal_out(jax.random.fold_in(arg_keys[2], 2), own, number, TOK_DEV, EXPERTS, 2, CAP, 1))(route_ids_keys, route_ids_turns).reshape((TOKENS, 2))
    route_weights = jnp.clip(0.1 + 0.79999997 * jax.random.uniform(arg_keys[3], (TOKENS, 2), jnp.float32) ** block_levels(arg_keys[3], (TOKENS, 2), ((0, 16),), -0.2, 0.2), 0.1, 0.9)
    gate_w = scatter_about(arg_keys[4], (2 * EXPERTS, D, FH), D ** -0.5, 0.125, ((0, 16), (2, 2)))
    up_w = scatter_about(arg_keys[5], (2 * EXPERTS, D, FH), D ** -0.5, 0.125, ((0, 16), (2, 2)))
    down_w = scatter_about(arg_keys[6], (2 * EXPERTS, FH, D), FFE ** -0.5, 0.09375, ((0, 16), (1, 2)))
    mixer_out = scatter_about(arg_keys[7], (TOKENS, HV), 1.0, 6.0, ((0, 16), (1, 2)))
    out_weight = scatter_about(arg_keys[8], (HV, D), HV ** -0.5, 0.1875, ((0, 2),))
    queries = scatter_about(arg_keys[9], (TOKENS, HK), 0.02, 0.125, ((0, 16), (1, 2)))
    keys = scatter_about(arg_keys[10], (TOKENS, HK), 0.05, 0.3125, ((0, 16), (1, 2)))
    values = scatter_about(arg_keys[11], (TOKENS, HV), 0.25, 1.5, ((0, 16), (1, 2)))
    log_decay = draw_log_decay(jax.random.fold_in(arg_keys[14], 71), 0)
    block_states = scatter_about(arg_keys[13], (NBLK, HEADS, DK, DV), 0.3, 1.75, ((0, 16), (1, 2)), jnp.float32)
    return dict(moe_input=moe_input, out_grad=out_grad, route_ids=route_ids, route_weights=route_weights, gate_w=gate_w, up_w=up_w, down_w=down_w, mixer_out=mixer_out, out_weight=out_weight, queries=queries, keys=keys, values=values, log_decay=log_decay, block_states=block_states)


PRECISE = lax.Precision.HIGHEST
ACROSS = (((1,), (1,)), ((), ()))
DOWNWARD = (((0,), (0,)), ((), ()))


def block_back(carried, inputs):
    q_block, k_block, v_block, o_block, decay_block, state_in = inputs
    cumul = jnp.cumsum(decay_block, axis=0)
    block_total = cumul[-1]
    growth = jnp.exp(cumul)
    shrink = jnp.exp(-cumul)
    to_end = jnp.exp(block_total[None] - cumul)
    span_len = q_block.shape[0]
    causal = (jnp.arange(span_len)[:, None] >= jnp.arange(span_len)[None, :]).astype(jnp.float32)
    q_grow = q_block * growth
    k_shrink = k_block * shrink
    scores = jnp.einsum('thv,shv->hts', o_block, v_block, precision=PRECISE) * causal
    mutual = jnp.einsum('thd,shd->hts', q_grow, k_shrink, precision=PRECISE) * causal
    grad_q = growth * (jnp.einsum('thv,hdv->thd', o_block, state_in, precision=PRECISE)
                       + jnp.einsum('hts,shd->thd', scores, k_shrink, precision=PRECISE))
    grad_k = to_end * jnp.einsum('hdv,shv->shd', carried, v_block, precision=PRECISE) \
        + shrink * jnp.einsum('hts,thd->shd', scores, q_grow, precision=PRECISE)
    grad_v = jnp.einsum('shd,hdv->shv', k_block * to_end, carried, precision=PRECISE) \
        + jnp.einsum('hts,thv->shv', mutual, o_block, precision=PRECISE)
    contrib = q_block * grad_q - k_block * grad_k
    carried = jnp.exp(block_total)[:, :, None] * carried + jnp.einsum('thd,thv->hdv', q_grow, o_block, precision=PRECISE)
    return carried, (grad_q, grad_k, grad_v, contrib)


def reference(moe_input, out_grad, route_ids, route_weights, gate_w, up_w, down_w, mixer_out,
              out_weight, queries, keys, values, log_decay, block_states):
    flat_ids = route_ids.reshape(-1).astype(jnp.int32)
    one_hot = (flat_ids[:, None] == jnp.arange(EXPERTS, dtype=jnp.int32)[None, :]).astype(jnp.int32)
    counted = jnp.cumsum(one_hot.reshape(N_SP, 2 * TOK_DEV, EXPERTS), axis=1).reshape(2 * TOKENS, EXPERTS)
    earlier_count = (jnp.sum(counted * one_hot, axis=1) - 1).astype(jnp.int32)
    source = (jnp.arange(2 * TOKENS, dtype=jnp.int32) // (2 * TOK_DEV)).astype(jnp.int32)
    slot_index = (source * CAP + earlier_count).astype(jnp.int32)
    table = jnp.full((EXPERTS, SLOTS), 2 * TOKENS, jnp.int32).at[flat_ids, slot_index].set(
        jnp.arange(2 * TOKENS, dtype=jnp.int32))
    token_rows = jnp.concatenate([jnp.repeat(moe_input, 2, axis=0), jnp.zeros((1, D), jnp.bfloat16)], axis=0)
    scaled = (route_weights[:, :, None] * out_grad[:, None, :].astype(jnp.float32)).astype(jnp.bfloat16)
    grad_rows = jnp.concatenate([scaled.reshape(2 * TOKENS, D), jnp.zeros((1, D), jnp.bfloat16)], axis=0)

    def expert_back(pieces):
        gate_pair, up_pair, down_pair, picks = pieces
        tokens_in = token_rows[picks]
        grads_in = grad_rows[picks]
        half_sums = []
        gate_halves, up_halves, down_halves = [], [], []
        for half in range(2):
            partial_value = jnp.zeros((SLOTS, D), jnp.float32)
            gate_parts, up_parts, down_parts = [], [], []
            for part in range(N_TP):
                w_gate = gate_pair[half][:, part * FQ:(part + 1) * FQ]
                w_up = up_pair[half][:, part * FQ:(part + 1) * FQ]
                w_down = down_pair[half][part * FQ:(part + 1) * FQ]
                gate_pre = jnp.dot(tokens_in, w_gate, preferred_element_type=jnp.float32)
                up_pre = jnp.dot(tokens_in, w_up, preferred_element_type=jnp.float32)
                sigmoid_gate = jax.nn.sigmoid(gate_pre)
                hidden = (gate_pre * sigmoid_gate * up_pre).astype(jnp.bfloat16)
                d_hidden = lax.dot_general(grads_in, w_down, ACROSS, preferred_element_type=jnp.float32)
                d_up = (d_hidden * gate_pre * sigmoid_gate).astype(jnp.bfloat16)
                d_gate = (d_hidden * up_pre * sigmoid_gate * (1.0 + gate_pre * (1.0 - sigmoid_gate))).astype(jnp.bfloat16)
                down_parts.append(lax.dot_general(hidden, grads_in, DOWNWARD, preferred_element_type=jnp.float32).astype(jnp.bfloat16))
                gate_parts.append(lax.dot_general(tokens_in, d_gate, DOWNWARD, preferred_element_type=jnp.float32).astype(jnp.bfloat16))
                up_parts.append(lax.dot_general(tokens_in, d_up, DOWNWARD, preferred_element_type=jnp.float32).astype(jnp.bfloat16))
                piece = lax.dot_general(d_gate, w_gate, ACROSS, preferred_element_type=jnp.float32) \
                    + lax.dot_general(d_up, w_up, ACROSS, preferred_element_type=jnp.float32)
                rounded = lax.optimization_barrier(piece.astype(jnp.bfloat16))
                partial_value = partial_value + rounded.astype(jnp.float32)
            half_sums.append(partial_value.astype(jnp.bfloat16))
            gate_halves.append(jnp.concatenate(gate_parts, axis=1))
            up_halves.append(jnp.concatenate(up_parts, axis=1))
            down_halves.append(jnp.concatenate(down_parts, axis=0))
        both_halves = half_sums[0].astype(jnp.float32) + half_sums[1].astype(jnp.float32)
        return both_halves, jnp.stack(gate_halves), jnp.stack(up_halves), jnp.stack(down_halves)

    returned, gate_grad, up_grad, down_grad = lax.map(
        expert_back,
        (gate_w.reshape(EXPERTS, 2, D, FH), up_w.reshape(EXPERTS, 2, D, FH),
         down_w.reshape(EXPERTS, 2, FH, D), table))
    routed = jnp.zeros((2 * TOKENS + 1, D), jnp.float32).at[table.reshape(-1)].add(returned.reshape(-1, D))
    moe_grad = jnp.sum(routed[:-1].reshape(TOKENS, 2, D), axis=1)
    grad_mid = (out_grad.astype(jnp.float32) + moe_grad).astype(jnp.bfloat16)
    grad_out_weight = lax.dot_general(mixer_out, grad_mid, DOWNWARD, preferred_element_type=jnp.float32)
    grad_mixed = lax.dot_general(grad_mid, out_weight, ACROSS, preferred_element_type=jnp.float32).astype(jnp.bfloat16)

    def shaped(array, depth):
        return array.astype(jnp.float32).reshape(NBLK, BLK, HEADS, depth)

    inputs = (shaped(queries, DK), shaped(keys, DK), shaped(values, DV), shaped(grad_mixed, DV),
              shaped(log_decay, DK), block_states)
    zero_state = jnp.zeros((HEADS, DK, DV), jnp.float32)
    _, (grad_q, grad_k, grad_v, contrib) = lax.scan(block_back, zero_state, inputs, reverse=True)
    contrib = contrib.reshape(TOKENS, HK)
    grad_decay = jnp.flip(jnp.cumsum(jnp.flip(contrib, 0), axis=0), 0)
    return (grad_q.reshape(TOKENS, HK).astype(jnp.bfloat16),
            grad_k.reshape(TOKENS, HK).astype(jnp.bfloat16),
            grad_v.reshape(TOKENS, HV).astype(jnp.bfloat16),
            grad_decay,
            grad_out_weight,
            gate_grad.reshape(2 * EXPERTS, D, FH),
            up_grad.reshape(2 * EXPERTS, D, FH),
            down_grad.reshape(2 * EXPERTS, FH, D))
```

```python
import functools

import jax
import jax.numpy as jnp
from jax import lax
from jax.experimental import pallas as pl
from jax.experimental.pallas import tpu as pltpu
from jax.sharding import Mesh, PartitionSpec as P

MESH = pl.DeviceIdType.MESH
SP = ("ep", "pair")

DK = 64
DV = 128
BLK = 64
PER_GROUP = 2


PRECISE = lax.Precision.HIGHEST
ACROSS = (((1,), (1,)), ((), ()))
DOWNWARD = (((0,), (0,)), ((), ()))
PLAIN = (((1,), (0,)), ((), ()))


def sp_size():
    return lax.axis_size("ep") * lax.axis_size("pair")


def sp_index():
    return lax.axis_index("ep") * lax.axis_size("pair") + lax.axis_index("pair")


def experts_kernel(
    experts, cap, ids, route_weights, moe_input, out_grad, gate_w, up_w, down_w,
    returned, gate_out, up_out, down_out,
    toks, grads, hidden, d_both, gate_up, down, silu_part, slope_part, parts, rank, tok_send,
    grad_send, core_held, pair_stage, pair_held, send_stage, gate_stage, up_stage, down_stage,
    weight_sem, out_sem, direct_send, direct_recv, pass_send, pass_recv, mate_send, mate_recv,
    core_send, core_recv, pair_send, pair_recv, back_send, back_recv,
):
    e, p, t = lax.axis_index("ep"), lax.axis_index("pair"), lax.axis_index("tp")
    f32, bf16 = jnp.float32, jnp.bfloat16
    tokens, model_width = moe_input.shape
    width = model_width // 2
    units = hidden.shape[1]
    group_rows = PER_GROUP * 2 * cap
    groups = experts // PER_GROUP
    pair_id, mate_id = (e, 1 - p, t), (e, p, 1 - t)
    barrier = pltpu.get_barrier_semaphore()
    for k in range(1, experts):
        pl.semaphore_signal(
            barrier, inc=1, device_id=(lax.rem(e + k, experts), p, t), device_id_type=MESH
        )
    pl.semaphore_signal(barrier, inc=1, device_id=pair_id, device_id_type=MESH)
    pl.semaphore_signal(barrier, inc=1, device_id=mate_id, device_id_type=MESH)
    loads = (
        pltpu.make_async_copy(gate_w, gate_up.at[:, pl.ds(0, units)], weight_sem.at[0]),
        pltpu.make_async_copy(up_w, gate_up.at[:, pl.ds(units, units)], weight_sem.at[1]),
        pltpu.make_async_copy(down_w, down, weight_sem.at[2]),
    )
    for load in loads:
        load.start()
    own_columns = pl.ds(pl.multiple_of(t * width, 128), width)
    core_columns = pl.ds(pl.multiple_of((1 - t) * width, 128), width)
    arrived = (toks, grads)
    sends = (tok_send, grad_send)

    def block(k, side):
        return pl.ds(pl.multiple_of((k * 2 + side) * cap, cap), cap)

    def remote(src, dst, send, recv, device):
        return pltpu.make_async_remote_copy(
            src_ref=src, dst_ref=dst, send_sem=send, recv_sem=recv, device_id=device,
            device_id_type=MESH,
        )

    def direct(a, k):
        return remote(
            sends[a].at[k], arrived[a].at[block(k, p), own_columns], direct_send.at[a, k],
            direct_recv.at[a, k], (lax.rem(e + k, experts), p, t),
        )

    def to_pair(a, k, side):
        place = arrived[a].at[block(k, side), own_columns]
        return remote(place, place, pass_send.at[a, k], pass_recv.at[a, k], pair_id)

    def to_mate(a, k, side, which, columns):
        place = arrived[a].at[block(k, side), columns]
        return remote(place, place, mate_send.at[a, which, k], mate_recv.at[a, which, k], mate_id)

    first_id, second_id = ids[0:1], ids[1:2]
    first_w, second_w = route_weights[0:1], route_weights[1:2]
    expert_row = lax.broadcasted_iota(jnp.int32, (experts, tokens), 0)
    member = (expert_row == first_id) | (expert_row == second_id)
    row = lax.broadcasted_iota(jnp.int32, (tokens, tokens), 0)
    col = lax.broadcasted_iota(jnp.int32, (tokens, tokens), 1)
    before = (row < col).astype(bf16)
    count = lax.dot_general(
        member.astype(f32).astype(bf16), before, PLAIN, preferred_element_type=f32
    )
    rank[...] = jnp.where(member, count.astype(jnp.int32), -1)
    spot = lax.broadcasted_iota(jnp.int32, (cap, tokens), 0)

    def rows_for(dest):
        pick = spot == rank[pl.ds(dest, 1)]
        weight = jnp.where(first_id == dest, first_w, second_w)
        scale = jnp.sum(jnp.where(pick, weight, 0.0), axis=1, keepdims=True)
        chosen = pick.astype(f32).astype(bf16)
        tok = lax.dot_general(chosen, moe_input[:, own_columns], PLAIN, preferred_element_type=f32)
        grad = lax.dot_general(chosen, out_grad[:, own_columns], PLAIN, preferred_element_type=f32)
        return tok.astype(bf16), (scale * grad).astype(bf16)

    own_tok, own_grad = rows_for(e)
    toks[block(0, p), own_columns] = own_tok
    grads[block(0, p), own_columns] = own_grad
    pl.semaphore_wait(barrier, experts + 1)
    for a in range(2):
        to_pair(a, 0, p).start()
        to_mate(a, 0, p, 0, own_columns).start()

    def send_step(k, carry):
        tok, grad = rows_for(lax.rem(e + k, experts))
        tok_send[k] = tok
        grad_send[k] = grad
        direct(0, k).start()
        direct(1, k).start()
        return carry

    lax.fori_loop(1, experts, send_step, 0)
    for load in loads:
        load.wait()

    def from_direct(a, k):
        @pl.when(k > 0)
        def _():
            direct(a, k).wait_recv()
            to_pair(a, k, p).start()
            to_mate(a, k, p, 0, own_columns).start()

    def from_pair(a, k):
        to_pair(a, k, 1 - p).wait_recv()
        to_mate(a, k, 1 - p, 1, own_columns).start()

    def from_mate(a, k):
        to_mate(a, k, p, 0, core_columns).wait_recv()
        to_mate(a, k, 1 - p, 1, core_columns).wait_recv()

    def core_copy(which, k):
        side = 1 - p if which == 0 else p
        return remote(
            parts.at[block(k, side), core_columns], core_held.at[which, k],
            core_send.at[which, k], core_recv.at[which, k], mate_id,
        )

    def pair_copy(k):
        return remote(
            pair_stage.at[k], pair_held.at[k], pair_send.at[k], pair_recv.at[k], pair_id
        )

    def back_copy(k):
        owner = lax.rem(e - k + experts, experts)
        return remote(
            send_stage.at[k], returned.at[e], back_send.at[k], back_recv.at[k], (owner, p, t)
        )

    def half_of(which, k):
        side = 1 - p if which == 0 else p
        mine = parts[block(k, side), own_columns].astype(f32)
        return (mine + core_held[which, k].astype(f32)).astype(bf16)

    def members(g):
        return [g * PER_GROUP + j for j in range(PER_GROUP)]

    def half_step(g):
        for k in members(g):
            core_copy(0, k).wait_recv()
            pair_stage[k] = half_of(0, k)
            pair_copy(k).start()

    def total_step(g):
        for k in members(g):
            core_copy(1, k).wait_recv()
            pair_copy(k).wait_recv()
            total = half_of(1, k).astype(f32) + pair_held[k].astype(f32)
            send_stage[k] = total.astype(bf16)

            @pl.when(k > 0)
            def _():
                back_copy(k).start()

    def group_step(g, carry):
        now, last = members(g), members(g - 1)
        rows = pl.ds(pl.multiple_of((g - 1) * group_rows, group_rows), group_rows)
        here, behind = g < groups, g > 0

        @pl.when(here)
        def _():
            for k in now:
                from_direct(0, k)

        @pl.when(behind)
        def _():
            for k in last:
                from_mate(0, k)
            gate_pre = lax.dot_general(
                toks[rows], gate_up[:, :units], PLAIN, preferred_element_type=f32
            )
            gate = jax.nn.sigmoid(gate_pre)
            silu_part[...] = gate_pre * gate
            slope_part[...] = gate * (1.0 + gate_pre * (1.0 - gate))

        @pl.when(here)
        def _():
            for k in now:
                from_direct(1, k)
                from_pair(0, k)

        @pl.when(behind)
        def _():
            up_pre = lax.dot_general(
                toks[rows], gate_up[:, units:], PLAIN, preferred_element_type=f32
            )
            hidden[rows] = (silu_part[...] * up_pre).astype(bf16)
            slope_part[...] = slope_part[...] * up_pre
            for k in last:
                from_mate(1, k)

        @pl.when(here)
        def _():
            for k in now:
                from_pair(1, k)

        @pl.when(behind)
        def _():
            d_hidden = lax.dot_general(grads[rows], down[...], ACROSS, preferred_element_type=f32)
            d_both[rows, :units] = (d_hidden * slope_part[...]).astype(bf16)
            d_both[rows, units:] = (d_hidden * silu_part[...]).astype(bf16)
            parts[rows, core_columns] = lax.dot_general(
                d_both[rows], gate_up[core_columns], ACROSS, preferred_element_type=f32
            ).astype(bf16)
            for k in last:
                core_copy(0, k).start()
                core_copy(1, k).start()

        @pl.when(g > 1)
        def _():
            total_step(g - 2)

        @pl.when(behind)
        def _():
            parts[rows, own_columns] = lax.dot_general(
                d_both[rows], gate_up[own_columns], ACROSS, preferred_element_type=f32
            ).astype(bf16)
            half_step(g - 1)

        return carry

    lax.fori_loop(0, groups + 1, group_step, 0)

    def down_step(i, carry):
        cut = pl.ds(pl.multiple_of(i * 128, 128), 128)
        down_stage[cut, :] = lax.dot_general(
            hidden[:, cut], grads[...], DOWNWARD, preferred_element_type=f32
        ).astype(bf16)
        pltpu.make_async_copy(down_stage.at[cut], down_out.at[cut], out_sem.at[0]).start()
        return carry

    lax.fori_loop(0, units // 128, down_step, 0)
    total_step(groups - 1)
    returned[e] = send_stage[0]

    def weight_step(i, carry):
        cut = pl.ds(pl.multiple_of(i * 256, 256), 256)
        both = lax.dot_general(
            toks[:, cut], d_both[...], DOWNWARD, preferred_element_type=f32
        ).astype(bf16)
        gate_stage[cut, :] = both[:, :units]
        up_stage[cut, :] = both[:, units:]
        pltpu.make_async_copy(gate_stage.at[cut], gate_out.at[cut], out_sem.at[1]).start()
        pltpu.make_async_copy(up_stage.at[cut], up_out.at[cut], out_sem.at[2]).start()
        return carry

    lax.fori_loop(0, model_width // 256, weight_step, 0)

    def close(k, carry):
        for a in range(2):
            to_pair(a, k, p).wait_send()
            to_mate(a, k, p, 0, own_columns).wait_send()
            to_mate(a, k, 1 - p, 1, own_columns).wait_send()
        core_copy(0, k).wait_send()
        core_copy(1, k).wait_send()
        pair_copy(k).wait_send()

        @pl.when(k > 0)
        def _():
            direct(0, k).wait_send()
            direct(1, k).wait_send()
            source = lax.rem(e + k, experts)
            remote(
                returned.at[source], returned.at[source], back_send.at[k], back_recv.at[k],
                (source, p, t),
            ).wait_recv()
            back_copy(k).wait_send()

        return carry

    lax.fori_loop(0, experts, close, 0)
    pltpu.make_async_copy(down_stage, down_out, out_sem.at[0]).wait()
    pltpu.make_async_copy(gate_stage, gate_out, out_sem.at[1]).wait()
    pltpu.make_async_copy(up_stage, up_out, out_sem.at[2]).wait()


def expert_rows(cap, ids, route_weights, moe_input, out_grad, gate_w, up_w, down_w):
    experts = lax.axis_size("ep")
    model_width, units = gate_w.shape
    width = model_width // lax.axis_size("tp")
    rows = experts * 2 * cap
    half = (experts, cap, width)
    vmem = pl.BlockSpec(memory_space=pltpu.VMEM)
    hbm = pl.BlockSpec(memory_space=pltpu.HBM)
    dma = pltpu.SemaphoreType.DMA
    wide, tall = (model_width, units), (units, model_width)
    kind, f32 = jnp.bfloat16, jnp.float32
    shape = jax.ShapeDtypeStruct
    group_rows = PER_GROUP * 2 * cap
    return pl.pallas_call(
        functools.partial(experts_kernel, experts, cap),
        out_shape=(shape(half, kind), shape(wide, kind), shape(wide, kind), shape(tall, kind)),
        in_specs=[vmem] * 4 + [hbm] * 3,
        out_specs=(vmem, hbm, hbm, hbm),
        scratch_shapes=[
            pltpu.VMEM((rows, model_width), kind),
            pltpu.VMEM((rows, model_width), kind),
            pltpu.VMEM((rows, units), kind),
            pltpu.VMEM((rows, 2 * units), kind),
            pltpu.VMEM((model_width, 2 * units), kind),
            pltpu.VMEM(tall, kind),
            pltpu.VMEM((group_rows, units), f32),
            pltpu.VMEM((group_rows, units), f32),
            pltpu.VMEM((rows, model_width), kind),
            pltpu.VMEM((experts, moe_input.shape[0]), jnp.int32),
            pltpu.VMEM(half, kind),
            pltpu.VMEM(half, kind),
            pltpu.VMEM((2,) + half, kind),
            pltpu.VMEM(half, kind),
            pltpu.VMEM(half, kind),
            pltpu.VMEM(half, kind),
            pltpu.VMEM(wide, kind),
            pltpu.VMEM(wide, kind),
            pltpu.VMEM(tall, kind),
            dma((3,)),
            dma((3,)),
            dma((2, experts)),
            dma((2, experts)),
            dma((2, experts)),
            dma((2, experts)),
            dma((2, 2, experts)),
            dma((2, 2, experts)),
            dma((2, experts)),
            dma((2, experts)),
            dma((experts,)),
            dma((experts,)),
            dma((experts,)),
            dma((experts,)),
        ],
        compiler_params=pltpu.CompilerParams(
            collective_id=0, has_side_effects=True, vmem_limit_bytes=60 * 1024 * 1024
        ),
        name="expert_rows",
    )(ids, route_weights, moe_input, out_grad, gate_w, up_w, down_w)


def attend_kernel(
    count, tp_count, rows, cap, ids, out_grad, returned, out_weight, queries, keys, values,
    log_decay, block_states,
    mid_columns, from_right, decay_dots, right_terms, grad_q, key_local, value_local, contrib_local,
    k_fade, fade_out,
    mid, mid_stage, early_stage, early_held, sum_stage, sum_held, result, dot_result, gathered,
    local_sem, mid_send, mid_recv, col_send, col_recv, pass_send, pass_recv,
    early_send, early_recv, sum_send, sum_recv, back_send, back_recv, dot_send, dot_recv,
    term_send, term_recv,
):
    me = sp_index()
    t = lax.axis_index("tp")
    tokens, channels = queries.shape
    heads = channels // DK
    blocks = tokens // BLK
    width = mid.shape[1] // tp_count
    share = count // tp_count
    f32, bf16 = jnp.float32, jnp.bfloat16

    def place(i, core):
        return (lax.div(i, 2), lax.rem(i, 2), core)

    barrier = pltpu.get_barrier_semaphore()
    for k in range(1, count):
        pl.semaphore_signal(
            barrier, inc=1, device_id=place(lax.rem(me + k, count), t), device_id_type=MESH
        )
    pl.semaphore_signal(barrier, inc=1, device_id=place(me, 1 - t), device_id_type=MESH)

    def dot(x, y, dims=(((1,), (0,)), ((), ()))):
        return lax.dot_general(
            x.astype(bf16), y.astype(bf16), dims, preferred_element_type=f32
        )

    def spread(src, dst, sends, recvs, k):
        dest = lax.rem(me + k, count)
        return pltpu.make_async_remote_copy(
            src_ref=src(dest), dst_ref=dst, send_sem=sends.at[k], recv_sem=recvs.at[k],
            device_id=place(dest, t), device_id_type=MESH,
        )

    def landed(ref, sends, recvs, k):
        source = lax.rem(me - k + count, count)
        pltpu.make_async_remote_copy(
            src_ref=ref.at[source], dst_ref=ref.at[source], send_sem=sends.at[k],
            recv_sem=recvs.at[k], device_id=place(source, t), device_id_type=MESH,
        ).wait_recv()

    row = lax.broadcasted_iota(jnp.int32, (tokens, tokens), 0)
    col = lax.broadcasted_iota(jnp.int32, (tokens, tokens), 1)
    earlier = (row >= col).astype(f32)
    decay = log_decay[...]
    position = lax.dot_general(
        earlier, decay, (((1,), (0,)), ((), ())), precision=PRECISE, preferred_element_type=f32
    )
    device_total = position[tokens - 1 :]
    fade = jnp.exp(device_total - position)
    k_all = keys[...].astype(f32)
    q_all = queries[...].astype(f32)
    v_all = values[...]
    faded = k_all * fade
    fade_out[...] = fade
    k_fade[...] = faded
    gain = jnp.transpose(jnp.broadcast_to(jnp.exp(device_total), (DV, channels)))

    for h in range(heads):
        ks, vs = slice(h * DK, (h + 1) * DK), slice(h * DV, (h + 1) * DV)
        reach = dot(faded[:, ks], v_all[:, vs], DOWNWARD)
        for j in range(DK // rows):
            cut = slice(j * rows, (j + 1) * rows)
            early_stage[h * (DK // rows) + j, 0] = reach[cut]
            early_stage[h * (DK // rows) + j, 1] = gain[h * DK + j * rows : h * DK + (j + 1) * rows]
    pl.semaphore_wait(barrier, count)
    early_held[me] = early_stage[me]
    for k in range(1, count):
        spread(lambda i: early_stage.at[i], early_held.at[me], early_send, early_recv, k).start()

    slot_count = returned.shape[0]
    expert_lane = lax.broadcasted_iota(jnp.int32, (tokens, slot_count // cap), 1)
    turned = [jnp.transpose(jnp.broadcast_to(ids[j : j + 1], (128, tokens))) for j in range(2)]
    first, second = expert_lane == turned[0][:, 0:1], expert_lane == turned[1][:, 0:1]
    rank = dot((row > col).astype(f32), (first | second).astype(f32)).astype(jnp.int32)
    spots = expert_lane * cap + rank
    slot_lane = lax.broadcasted_iota(jnp.int32, (tokens, slot_count), 1)
    first_slot = jnp.sum(jnp.where(first, spots, 0), axis=1, keepdims=True)
    second_slot = jnp.sum(jnp.where(second, spots, 0), axis=1, keepdims=True)
    pick = (slot_lane == first_slot) | (slot_lane == second_slot)
    own_columns = pl.ds(pl.multiple_of(t * width, 128), width)
    core_columns = pl.ds(pl.multiple_of((1 - t) * width, 128), width)
    moe = dot(pick.astype(f32), returned[...])
    mid_half = (out_grad[:, own_columns].astype(f32) + moe).astype(bf16)
    mid[:, own_columns] = mid_half

    def to_core(columns):
        return pltpu.make_async_remote_copy(
            src_ref=mid.at[:, columns], dst_ref=mid.at[:, columns], send_sem=mid_send,
            recv_sem=mid_recv, device_id=place(me, 1 - t), device_id_type=MESH,
        )

    to_core(own_columns).start()
    piece = width // share
    for j in range(share):
        mid_stage[j] = mid_half[:, j * piece : (j + 1) * piece]

    cumul = [position[:BLK]]
    for n in range(1, blocks):
        cumul.append(position[n * BLK : (n + 1) * BLK] - position[n * BLK - 1 : n * BLK])
    growth = [jnp.exp(c) for c in cumul]
    shrink = [jnp.exp(-c) for c in cumul]
    to_end = [jnp.exp(c[BLK - 1 :] - c) for c in cumul]
    span = [slice(n * BLK, (n + 1) * BLK) for n in range(blocks)]
    q_grow = [(q_all[span[n]] * growth[n]).astype(bf16) for n in range(blocks)]
    k_shrink = [(k_all[span[n]] * shrink[n]).astype(bf16) for n in range(blocks)]
    k_end = [(k_all[span[n]] * to_end[n]).astype(bf16) for n in range(blocks)]
    q_long = (q_all * jnp.exp(position)).astype(bf16)

    to_core(core_columns).wait_recv()
    o_all = dot(mid[...], out_weight[...], ACROSS).astype(bf16)
    for h in range(heads):
        ks, vs = slice(h * DK, (h + 1) * DK), slice(h * DV, (h + 1) * DV)
        summed = dot(q_long[:, ks], o_all[:, vs], DOWNWARD)
        for j in range(DK // rows):
            sum_stage[h * (DK // rows) + j] = summed[j * rows : (j + 1) * rows]
    sum_held[me] = sum_stage[me]
    for k in range(1, count):
        spread(lambda i: sum_stage.at[i], sum_held.at[me], sum_send, sum_recv, k).start()

    def own_share(c):
        return lax.div(c, share) == t

    def column_copy(j):
        dest = t * share + lax.rem(me + j, share)
        return pltpu.make_async_remote_copy(
            src_ref=mid_stage.at[lax.rem(me + j, share)], dst_ref=mid_columns.at[me],
            send_sem=col_send.at[j], recv_sem=col_recv.at[lax.rem(dest - me + count, count)],
            device_id=place(dest, t), device_id_type=MESH,
        )

    def column_self(c):
        return pltpu.make_async_copy(
            mid_stage.at[lax.rem(c, share)], mid_columns.at[c], local_sem
        )

    for j in range(share):

        @pl.when(t * share + lax.rem(me + j, share) != me)
        def _():
            column_copy(j).start()

    @pl.when(own_share(me))
    def _():
        column_self(me).start()

    lane_causal = row[:BLK, :BLK] >= col[:BLK, :BLK]
    lane_causal_t = row[:BLK, :BLK] <= col[:BLK, :BLK]
    for n in range(blocks - 1, -1, -1):
        for h in range(heads):
            ks, vs = slice(h * DK, (h + 1) * DK), slice(h * DV, (h + 1) * DV)
            o, v = o_all[span[n], vs], v_all[span[n], vs]
            qg, kk = q_grow[n][:, ks], k_shrink[n][:, ks]
            state_in = block_states[n, h].astype(bf16)
            scores = jnp.where(lane_causal, dot(o, v, ACROSS), 0.0)
            scores_t = jnp.where(lane_causal_t, dot(v, o, ACROSS), 0.0)
            mutual_t = jnp.where(lane_causal_t, dot(kk, qg, ACROSS), 0.0)
            gq = growth[n][:, ks] * (dot(o, state_in, ACROSS) + dot(scores, kk))
            gk = shrink[n][:, ks] * dot(scores_t, qg)
            gv = dot(mutual_t, o)
            if n < blocks - 1:
                later = slice((n + 1) * BLK, tokens)
                end = position[(n + 1) * BLK - 1 : (n + 1) * BLK, ks]
                carried = dot(
                    q_all[later, ks] * jnp.exp(position[later, ks] - end), o_all[later, vs], DOWNWARD
                )
                gk = gk + to_end[n][:, ks] * dot(v, carried, ACROSS)
                gv = gv + dot(k_end[n][:, ks], carried)
            grad_q[span[n], ks] = gq
            key_local[span[n], ks] = gk
            value_local[span[n], vs] = gv
    contrib = q_all * grad_q[...] - k_all * key_local[...]
    contrib_local[...] = contrib
    gathered[me] = jnp.sum(contrib, axis=0, keepdims=True)
    for k in range(1, count):
        spread(lambda i: gathered.at[me], gathered.at[me], term_send, term_recv, k).start()

    for k in range(1, count):
        landed(early_held, early_send, early_recv, k)
    for k in range(1, count):
        landed(sum_held, sum_send, sum_recv, k)
    total = jnp.zeros((rows, DV), f32)
    dots = jnp.zeros((rows, DV), f32)
    for i in range(count - 1, -1, -1):
        result[i] = total
        dot_result[i] = dots
        reach_dot = jnp.sum(early_held[i, 0] * total, axis=1, keepdims=True)
        dots = dots + jnp.broadcast_to(reach_dot, (rows, DV))
        total = early_held[i, 1] * total + sum_held[i]
    from_right[me] = result[me]
    decay_dots[me] = dot_result[me]
    for k in range(1, count):
        spread(lambda i: result.at[i], from_right.at[me], back_send, back_recv, k).start()
    for k in range(1, count):
        spread(lambda i: dot_result.at[i], decay_dots.at[me], dot_send, dot_recv, k).start()

    def pass_copy(c, index):
        return pltpu.make_async_remote_copy(
            src_ref=mid_columns.at[c], dst_ref=mid_columns.at[c], send_sem=pass_send.at[index],
            recv_sem=pass_recv.at[index], device_id=place(me, 1 - t), device_id_type=MESH,
        )

    @pl.when(own_share(me))
    def _():
        column_self(me).wait()
        pass_copy(me, 0).start()
        for k in range(1, count):
            landed(mid_columns, pass_send, col_recv, k)
            pass_copy(lax.rem(me - k + count, count), k).start()

    @pl.when(jnp.logical_not(own_share(me)))
    def _():
        for k in range(count):
            pass_copy(lax.rem(me - k + count, count), k).wait_recv()

    for k in range(1, count):
        landed(gathered, term_send, term_recv, k)
    summed_terms = jnp.zeros((1, channels), f32)
    for i in range(count):
        summed_terms += jnp.where(i > me, gathered[i], 0.0)
    right_terms[...] = summed_terms
    for k in range(1, count):
        landed(from_right, back_send, back_recv, k)
        landed(decay_dots, dot_send, dot_recv, k)
    to_core(own_columns).wait_send()
    for j in range(share):

        @pl.when(t * share + lax.rem(me + j, share) != me)
        def _():
            column_copy(j).wait_send()

    @pl.when(own_share(me))
    def _():
        for k in range(count):
            pass_copy(lax.rem(me - k + count, count), k).wait_send()

    for k in range(1, count):
        spread(lambda i: early_stage.at[i], early_held.at[me], early_send, early_recv, k).wait_send()
        spread(lambda i: sum_stage.at[i], sum_held.at[me], sum_send, sum_recv, k).wait_send()
        spread(lambda i: result.at[i], from_right.at[me], back_send, back_recv, k).wait_send()
        spread(lambda i: dot_result.at[i], decay_dots.at[me], dot_send, dot_recv, k).wait_send()
        spread(lambda i: gathered.at[me], gathered.at[me], term_send, term_recv, k).wait_send()


def attend(cap, ids, out_grad, returned, out_weight, queries, keys, values, log_decay, block_states):
    count = sp_size()
    tp_count = lax.axis_size("tp")
    tokens, channels = queries.shape
    model_width = out_grad.shape[1]
    heads = channels // DK
    rows = channels // count
    share = count // tp_count
    piece = model_width // count
    f32, bf16 = jnp.float32, jnp.bfloat16
    vmem = pl.BlockSpec(memory_space=pltpu.VMEM)
    dma = pltpu.SemaphoreType.DMA
    shape = jax.ShapeDtypeStruct
    wide = shape((tokens, channels), f32)
    return pl.pallas_call(
        functools.partial(attend_kernel, count, tp_count, rows, cap),
        out_shape=(
            shape((count, tokens, piece), bf16),
            shape((count, rows, DV), f32),
            shape((count, rows, DV), f32),
            shape((1, channels), f32),
            wide,
            wide,
            shape((tokens, heads * DV), f32),
            wide,
            wide,
            wide,
        ),
        in_specs=[vmem] * 9,
        out_specs=(vmem,) * 10,
        scratch_shapes=[
            pltpu.VMEM((tokens, model_width), bf16),
            pltpu.VMEM((share, tokens, piece), bf16),
            pltpu.VMEM((count, 2, rows, DV), f32),
            pltpu.VMEM((count, 2, rows, DV), f32),
            pltpu.VMEM((count, rows, DV), f32),
            pltpu.VMEM((count, rows, DV), f32),
            pltpu.VMEM((count, rows, DV), f32),
            pltpu.VMEM((count, rows, DV), f32),
            pltpu.VMEM((count, 1, channels), f32),
            dma,
            dma,
            dma,
            dma((share,)),
            dma((count,)),
            dma((count,)),
            dma((count,)),
            dma((count,)),
            dma((count,)),
            dma((count,)),
            dma((count,)),
            dma((count,)),
            dma((count,)),
            dma((count,)),
            dma((count,)),
            dma((count,)),
            dma((count,)),
        ],
        compiler_params=pltpu.CompilerParams(
            collective_id=1, has_side_effects=True, vmem_limit_bytes=60 * 1024 * 1024
        ),
        name="attend",
    )(ids, out_grad, returned, out_weight, queries, keys, values, log_decay, block_states)


def finish_kernel(
    chunks, mixer, mid_columns, from_right, decay_dots, right_terms, query_local, key_local,
    value_local, contrib_local, k_fade, fade_out, values, weight_a, weight_b, weight_c,
    grad_q, grad_k, grad_v, grad_decay, grad_out, out_a, out_b, out_c,
    hold_a, hold_b, hold_c, in_sem, out_sem,
):
    f32, bf16 = jnp.float32, jnp.bfloat16
    trios = ((weight_a, hold_a, out_a), (weight_b, hold_b, out_b), (weight_c, hold_c, out_c))

    def moves(a, j):
        source, hold, target = trios[a]
        size = source.shape[0] // chunks
        cut = pl.ds(j * size, size)
        return (
            pltpu.make_async_copy(source.at[cut], hold.at[cut], in_sem.at[a, j]),
            pltpu.make_async_copy(hold.at[cut], target.at[cut], out_sem.at[a, j]),
        )

    steps = [(a, j) for a in range(3) for j in range(chunks)]
    for a, j in steps:
        moves(a, j)[0].start()

    def dot(x, y, dims=(((1,), (0,)), ((), ()))):
        return lax.dot_general(
            x.astype(bf16), y.astype(bf16), dims, preferred_element_type=f32
        )

    def forward(group):
        for a, j in group:
            moves(a, j)[0].wait()
            moves(a, j)[1].start()

    tokens, channels = key_local.shape
    heads = channels // DK
    grad_q[...] = query_local[...].astype(bf16)
    forward(steps[:chunks])
    key_parts = []
    for h in range(heads):
        ks, vs = slice(h * DK, (h + 1) * DK), slice(h * DV, (h + 1) * DV)
        carried = from_right[h].astype(bf16)
        key_parts.append(dot(values[:, vs], carried, ACROSS))
        grad_v[:, vs] = (value_local[:, vs] + dot(k_fade[:, ks], carried)).astype(bf16)
    key_part = jnp.concatenate(key_parts, axis=1)
    grad_k[...] = (key_local[...] + fade_out[...] * key_part).astype(bf16)
    contrib = contrib_local[...] - k_fade[...] * key_part
    forward(steps[chunks : 2 * chunks])
    row = lax.broadcasted_iota(jnp.int32, (tokens, tokens), 0)
    col = lax.broadcasted_iota(jnp.int32, (tokens, tokens), 1)
    later = (col >= row).astype(f32)
    groups = []
    spot = lax.broadcasted_iota(jnp.int32, (128, 128), 0)
    lane = lax.broadcasted_iota(jnp.int32, (128, 128), 1)
    for g in range(channels // 128):
        picked = jnp.where(spot == lane, decay_dots[g * 128 : (g + 1) * 128], 0.0)
        groups.append(jnp.sum(picked, axis=0, keepdims=True))
    right = right_terms[...] - jnp.concatenate(groups, axis=1)
    grad_decay[...] = right + lax.dot_general(
        later, contrib, (((1,), (0,)), ((), ())), precision=PRECISE, preferred_element_type=f32
    )
    grad_out[...] = dot(mixer[...], mid_columns[...], DOWNWARD)
    forward(steps[2 * chunks :])
    for a, j in steps:
        moves(a, j)[1].wait()


def finish(mixer, local, values, weights):
    mid_columns, from_right, decay_dots, right_terms, *rest = local
    tokens, channels = rest[1].shape
    heads = channels // DK
    mid_columns = mid_columns.reshape(mixer.shape[0], -1)
    from_right = from_right.reshape(heads, DK, DV)
    decay_dots = decay_dots.reshape(channels, DV)
    vmem = pl.BlockSpec(memory_space=pltpu.VMEM)
    hbm = pl.BlockSpec(memory_space=pltpu.HBM)
    dma = pltpu.SemaphoreType.DMA
    shape = jax.ShapeDtypeStruct
    f32, bf16 = jnp.float32, jnp.bfloat16
    chunks = 4
    return pl.pallas_call(
        functools.partial(finish_kernel, chunks),
        out_shape=(
            shape((tokens, channels), bf16),
            shape((tokens, channels), bf16),
            shape((tokens, heads * DV), bf16),
            shape((tokens, channels), f32),
            shape((mixer.shape[1], mid_columns.shape[1]), f32),
            *(shape(w.shape, w.dtype) for w in weights),
        ),
        in_specs=[vmem] * 12 + [hbm] * 3,
        out_specs=(vmem,) * 5 + (hbm,) * 3,
        scratch_shapes=[pltpu.VMEM(w.shape, w.dtype) for w in weights]
        + [dma((3, chunks)), dma((3, chunks))],
        compiler_params=pltpu.CompilerParams(vmem_limit_bytes=60 * 1024 * 1024),
        name="finish",
    )(mixer, mid_columns, from_right, decay_dots, right_terms, *rest, values, *weights)


def body(
    moe_input,
    out_grad,
    route_ids,
    route_weights,
    gate_w,
    up_w,
    down_w,
    mixer_out,
    out_weight,
    queries,
    keys,
    values,
    log_decay,
    block_states,
):
    experts = lax.axis_size("ep")
    cap = -(-3 * moe_input.shape[0] // experts // 16) * 16
    returned, *weights = expert_rows(
        cap, route_ids.T, route_weights.T, moe_input, out_grad, gate_w[0], up_w[0], down_w[0]
    )
    mixer_all = lax.all_gather(mixer_out, SP, axis=0, tiled=True)
    local = attend(
        cap, route_ids.T, out_grad, returned.reshape(experts * cap, -1), out_weight, queries, keys,
        values, log_decay, block_states,
    )
    grad_q, grad_k, grad_v, grad_decay, grad_out_weight, grad_gate, grad_up, grad_down = finish(
        mixer_all, local, values, weights
    )
    return (
        grad_q,
        grad_k,
        grad_v,
        grad_decay,
        grad_out_weight,
        grad_gate[None],
        grad_up[None],
        grad_down[None],
    )


def solution(mesh):
    sp_count, tp_count = mesh.devices.shape
    mesh = Mesh(mesh.devices.reshape(sp_count // 2, 2, tp_count), ("ep", "pair", "tp"))
    placed = (
        P(SP, None),
        P(SP, None),
        P(SP, None),
        P(SP, None),
        P(SP, None, "tp"),
        P(SP, None, "tp"),
        P(SP, "tp", None),
        P(SP, "tp"),
        P("tp", None),
        P(SP, "tp"),
        P(SP, "tp"),
        P(SP, "tp"),
        P(SP, "tp"),
        P(SP, "tp", None, None),
    )
    return jax.shard_map(
        body,
        mesh=mesh,
        in_specs=placed,
        out_specs=(
            P(SP, "tp"),
            P(SP, "tp"),
            P(SP, "tp"),
            P(SP, "tp"),
            P("tp", SP),
            P(SP, None, "tp"),
            P(SP, None, "tp"),
            P(SP, "tp", None),
        ),
        check_vma=False,
    )
```

```python
import functools

import jax
import jax.numpy as jnp
from jax import lax
from jax.experimental import pallas as pl
from jax.experimental.pallas import tpu as pltpu
from jax.sharding import Mesh, PartitionSpec as P

MESH = pl.DeviceIdType.MESH
SP = ("ep", "pair")

DK = 64
DV = 128
BLK = 64
PER_GROUP = 2


PRECISE = lax.Precision.HIGHEST
ACROSS = (((1,), (1,)), ((), ()))
DOWNWARD = (((0,), (0,)), ((), ()))
PLAIN = (((1,), (0,)), ((), ()))


def sp_size():
    return lax.axis_size("ep") * lax.axis_size("pair")


def sp_index():
    return lax.axis_index("ep") * lax.axis_size("pair") + lax.axis_index("pair")


def experts_kernel(
    experts, cap, ids, route_weights, moe_input, out_grad, gate_w, up_w, down_w,
    mixer_hbm, out_weight_hbm, queries_hbm, keys_hbm, values_hbm, log_decay_hbm, block_states_hbm,
    gate_out, up_out, down_out, grad_out, from_right, decay_dots, right_terms, grad_q, key_local,
    value_local, contrib_local, k_fade, fade_out,
    out_weight, queries, keys, values, log_decay, block_states, mixers, returned, position_ref,
    mid, mid_stage, mid_columns, early_stage, early_held, sum_stage, sum_held, result, dot_result,
    gathered, near_part, near_held,
    toks, grads, hidden, d_both, gate_up, down, silu_part, slope_part, parts, rank, tok_send,
    grad_send, core_held, pair_stage, pair_held, send_stage, gate_stage, up_stage, down_stage,
    weight_sem, out_sem, direct_send, direct_recv, pass_send, pass_recv, mate_send, mate_recv,
    core_send, core_recv, pair_send, pair_recv, back_send, back_recv,
    load_sem, mixer_send, mixer_recv, side_send, side_recv, mid_send, mid_recv, col_send, col_recv,
    cross_send, cross_recv, near_send, near_recv, early_send, early_recv, sum_send, sum_recv,
    right_send, right_recv, dot_send, dot_recv, term_send, term_recv,
):
    e, p, t = lax.axis_index("ep"), lax.axis_index("pair"), lax.axis_index("tp")
    f32, bf16 = jnp.float32, jnp.bfloat16
    tokens, model_width = moe_input.shape
    width = model_width // 2
    units = hidden.shape[1]
    group_rows = PER_GROUP * 2 * cap
    groups = experts // PER_GROUP
    pair_id, mate_id = (e, 1 - p, t), (e, p, 1 - t)
    barrier = pltpu.get_barrier_semaphore()
    me = e * 2 + p
    count = experts * 2
    half_experts = experts // 2
    low, high = lax.rem(e, 2), lax.div(e, 2)
    here = high * 2 + p

    def place(i):
        return (lax.div(i, 2), lax.rem(i, 2), t)

    for k in range(1, count):
        pl.semaphore_signal(
            barrier, inc=1, device_id=place(lax.rem(me + k, count)), device_id_type=MESH
        )
    pl.semaphore_signal(barrier, inc=1, device_id=mate_id, device_id_type=MESH)

    def flip(k):
        total, bit = 0, 1
        while bit < experts:
            other = k // bit if isinstance(k, int) else lax.div(k, bit)
            total = total + bit * lax.rem(lax.div(e, bit) + other, 2)
            bit *= 2
        return total

    own_mixer = pltpu.make_async_copy(mixer_hbm, mixers.at[here], load_sem.at[6])
    late = [
        pltpu.make_async_copy(src, dst, load_sem.at[i])
        for i, (src, dst) in enumerate(
            (
                (log_decay_hbm, log_decay),
                (keys_hbm, keys),
                (values_hbm, values),
                (queries_hbm, queries),
                (out_weight_hbm, out_weight),
                (block_states_hbm, block_states),
            )
        )
    ]
    loads = (
        pltpu.make_async_copy(gate_w, gate_up.at[:, pl.ds(0, units)], weight_sem.at[0]),
        pltpu.make_async_copy(up_w, gate_up.at[:, pl.ds(units, units)], weight_sem.at[1]),
        pltpu.make_async_copy(down_w, down, weight_sem.at[2]),
    )
    for load in late[:3] + list(loads) + late[3:] + [own_mixer]:
        load.start()
    own_columns = pl.ds(pl.multiple_of(t * width, 128), width)
    core_columns = pl.ds(pl.multiple_of((1 - t) * width, 128), width)
    arrived = (toks, grads)
    sends = (tok_send, grad_send)

    def block(k, side):
        return pl.ds(pl.multiple_of((k * 2 + side) * cap, cap), cap)

    def remote(src, dst, send, recv, device):
        return pltpu.make_async_remote_copy(
            src_ref=src, dst_ref=dst, send_sem=send, recv_sem=recv, device_id=device,
            device_id_type=MESH,
        )

    def direct(a, k):
        return remote(
            sends[a].at[k], arrived[a].at[block(k, p), own_columns], direct_send.at[a, k],
            direct_recv.at[a, k], (flip(k), p, t),
        )

    def to_pair(a, k, side):
        place = arrived[a].at[block(k, side), own_columns]
        return remote(place, place, pass_send.at[a, k], pass_recv.at[a, k], pair_id)

    def to_mate(a, k, side, which, columns):
        place = arrived[a].at[block(k, side), columns]
        return remote(place, place, mate_send.at[a, which, k], mate_recv.at[a, which, k], mate_id)

    first_id, second_id = ids[0:1], ids[1:2]
    first_w, second_w = route_weights[0:1], route_weights[1:2]
    expert_row = lax.broadcasted_iota(jnp.int32, (experts, tokens), 0)
    member = (expert_row == first_id) | (expert_row == second_id)
    row = lax.broadcasted_iota(jnp.int32, (tokens, tokens), 0)
    col = lax.broadcasted_iota(jnp.int32, (tokens, tokens), 1)
    before = (row < col).astype(bf16)
    earlier = lax.dot_general(
        member.astype(f32).astype(bf16), before, PLAIN, preferred_element_type=f32
    )
    rank[...] = jnp.where(member, earlier.astype(jnp.int32), -1)
    spot = lax.broadcasted_iota(jnp.int32, (cap, tokens), 0)

    def rows_for(dest):
        pick = spot == rank[pl.ds(dest, 1)]
        weight = jnp.where(first_id == dest, first_w, second_w)
        scale = jnp.sum(jnp.where(pick, weight, 0.0), axis=1, keepdims=True)
        chosen = pick.astype(f32).astype(bf16)
        tok = lax.dot_general(chosen, moe_input[:, own_columns], PLAIN, preferred_element_type=f32)
        grad = lax.dot_general(chosen, out_grad[:, own_columns], PLAIN, preferred_element_type=f32)
        return tok.astype(bf16), (scale * grad).astype(bf16)

    own_tok, own_grad = rows_for(e)
    toks[block(0, p), own_columns] = own_tok
    grads[block(0, p), own_columns] = own_grad
    pl.semaphore_wait(barrier, count)
    for a in range(2):
        to_pair(a, 0, p).start()
        to_mate(a, 0, p, 0, own_columns).start()

    def send_step(k, carry):
        tok, grad = rows_for(flip(k))
        tok_send[k] = tok
        grad_send[k] = grad
        direct(0, k).start()
        direct(1, k).start()
        return carry

    lax.fori_loop(1, experts, send_step, 0)

    def mixer_copy(k):
        dest = lax.rem(high + k, half_experts) * 2 + low
        return remote(
            mixer_hbm, mixers.at[here], mixer_send.at[k], mixer_recv.at[k], (dest, p, t)
        )

    def mixer_place(k, side):
        return mixers.at[lax.rem(high - k + half_experts, half_experts) * 2 + side]

    def mixer_landed(k):
        spot = mixer_place(k, p)
        remote(spot, spot, mixer_send.at[k], mixer_recv.at[k], pair_id).wait_recv()

    def mixer_side(k, side):
        spot = mixer_place(k, side)
        return remote(spot, spot, side_send.at[k], side_recv.at[k], pair_id)

    for k in range(1, half_experts):
        mixer_copy(k).start()

    channels = queries.shape[1]
    heads = channels // DK
    blocks = tokens // BLK
    rows = channels // count
    per_head = DK // rows

    def dot(x, y, dims=PLAIN):
        return lax.dot_general(
            x.astype(bf16), y.astype(bf16), dims, preferred_element_type=f32
        )

    def spread(src, dst, sends, recvs, k):
        dest = lax.rem(me + k, count)
        return remote(src(dest), dst, sends.at[k], recvs.at[k], place(dest))

    def landed(ref, sends, recvs, k):
        source = lax.rem(me - k + count, count)
        remote(ref.at[source], ref.at[source], sends.at[k], recvs.at[k], place(source)).wait_recv()

    def early_copy(k):
        return spread(lambda i: early_stage.at[i], early_held.at[me], early_send, early_recv, k)

    for load in late[:3]:
        load.wait()
    position_ref[...] = lax.dot_general(
        (row >= col).astype(f32), log_decay[...], PLAIN, precision=PRECISE,
        preferred_element_type=f32,
    )
    device_total = position_ref[tokens - 1 :]
    fade = jnp.exp(device_total - position_ref[...])
    faded = keys[...].astype(f32) * fade
    fade_out[...] = fade
    k_fade[...] = faded
    gain = jnp.transpose(jnp.broadcast_to(jnp.exp(device_total), (DV, channels)))
    for h in range(heads):
        ks, vs = slice(h * DK, (h + 1) * DK), slice(h * DV, (h + 1) * DV)
        reach = dot(faded[:, ks], values[:, vs], DOWNWARD)
        for j in range(per_head):
            early_stage[h * per_head + j, 0] = reach[j * rows : (j + 1) * rows]
            early_stage[h * per_head + j, 1] = gain[h * DK + j * rows : h * DK + (j + 1) * rows]
    early_held[me] = early_stage[me]
    for k in range(1, count):
        early_copy(k).start()
    for load in loads:
        load.wait()

    def from_direct(a, k):
        @pl.when(k > 0)
        def _():
            direct(a, k).wait_recv()
            to_pair(a, k, p).start()
            to_mate(a, k, p, 0, own_columns).start()

    def from_pair(a, k):
        to_pair(a, k, 1 - p).wait_recv()
        to_mate(a, k, 1 - p, 1, own_columns).start()

    def from_mate(a, k):
        to_mate(a, k, p, 0, core_columns).wait_recv()
        to_mate(a, k, 1 - p, 1, core_columns).wait_recv()

    def core_copy(which, k):
        side = 1 - p if which == 0 else p
        return remote(
            parts.at[block(k, side), core_columns], core_held.at[which, k],
            core_send.at[which, k], core_recv.at[which, k], mate_id,
        )

    def pair_copy(k):
        return remote(
            pair_stage.at[k], pair_held.at[k], pair_send.at[k], pair_recv.at[k], pair_id
        )

    def back_copy(k):
        return remote(
            send_stage.at[k], returned.at[pl.ds(pl.multiple_of(e * cap, cap), cap)], back_send.at[k], back_recv.at[k], (flip(k), p, t)
        )

    def half_of(which, k):
        side = 1 - p if which == 0 else p
        mine = parts[block(k, side), own_columns].astype(f32)
        return (mine + core_held[which, k].astype(f32)).astype(bf16)

    def members(g):
        return [g * PER_GROUP + j for j in range(PER_GROUP)]

    def half_step(g):
        for k in members(g):
            core_copy(0, k).wait_recv()
            pair_stage[k] = half_of(0, k)
            pair_copy(k).start()

    def total_step(g):
        for k in members(g):
            core_copy(1, k).wait_recv()
            pair_copy(k).wait_recv()
            total = half_of(1, k).astype(f32) + pair_held[k].astype(f32)
            send_stage[k] = total.astype(bf16)

            @pl.when(k > 0)
            def _():
                back_copy(k).start()

    def group_step(g, carry):
        now, last = members(g), members(g - 1)
        rows = pl.ds(pl.multiple_of((g - 1) * group_rows, group_rows), group_rows)
        coming, behind = g < groups, g > 0

        @pl.when(coming)
        def _():
            for k in now:
                from_direct(0, k)

        @pl.when(behind)
        def _():
            for k in last:
                from_mate(0, k)
            gate_pre = lax.dot_general(
                toks[rows], gate_up[:, :units], PLAIN, preferred_element_type=f32
            )
            gate = jax.nn.sigmoid(gate_pre)
            silu_part[...] = gate_pre * gate
            slope_part[...] = gate * (1.0 + gate_pre * (1.0 - gate))

        @pl.when(coming)
        def _():
            for k in now:
                from_direct(1, k)
                from_pair(0, k)

        @pl.when(behind)
        def _():
            up_pre = lax.dot_general(
                toks[rows], gate_up[:, units:], PLAIN, preferred_element_type=f32
            )
            hidden[rows] = (silu_part[...] * up_pre).astype(bf16)
            slope_part[...] = slope_part[...] * up_pre
            for k in last:
                from_mate(1, k)

        @pl.when(coming)
        def _():
            for k in now:
                from_pair(1, k)

        @pl.when(behind)
        def _():
            d_hidden = lax.dot_general(grads[rows], down[...], ACROSS, preferred_element_type=f32)
            d_both[rows, :units] = (d_hidden * slope_part[...]).astype(bf16)
            d_both[rows, units:] = (d_hidden * silu_part[...]).astype(bf16)
            parts[rows, core_columns] = lax.dot_general(
                d_both[rows], gate_up[core_columns], ACROSS, preferred_element_type=f32
            ).astype(bf16)
            for k in last:
                core_copy(0, k).start()
                core_copy(1, k).start()

        @pl.when(g > 1)
        def _():
            total_step(g - 2)

        @pl.when(behind)
        def _():
            parts[rows, own_columns] = lax.dot_general(
                d_both[rows], gate_up[own_columns], ACROSS, preferred_element_type=f32
            ).astype(bf16)
            half_step(g - 1)

        return carry

    lax.fori_loop(0, groups + 1, group_step, 0)

    def down_step(i, carry):
        cut = pl.ds(pl.multiple_of(i * 128, 128), 128)
        down_stage[cut, :] = lax.dot_general(
            hidden[:, cut], grads[...], DOWNWARD, preferred_element_type=f32
        ).astype(bf16)
        pltpu.make_async_copy(down_stage.at[cut], down_out.at[cut], out_sem.at[0]).start()
        return carry

    def weight_step(i, carry):
        cut = pl.ds(pl.multiple_of(i * 256, 256), 256)
        both = lax.dot_general(
            toks[:, cut], d_both[...], DOWNWARD, preferred_element_type=f32
        ).astype(bf16)
        gate_stage[cut, :] = both[:, :units]
        up_stage[cut, :] = both[:, units:]
        pltpu.make_async_copy(gate_stage.at[cut], gate_out.at[cut], out_sem.at[1]).start()
        pltpu.make_async_copy(up_stage.at[cut], up_out.at[cut], out_sem.at[2]).start()
        return carry

    weight_steps = model_width // 256
    first_cut, second_cut = weight_steps // 4, weight_steps // 2
    own_mixer.wait()
    mixer_side(0, p).start()
    for k in range(1, half_experts):
        mixer_landed(k)
        mixer_side(k, p).start()
    lax.fori_loop(0, units // 128, down_step, 0)
    total_step(groups - 1)
    returned[pl.ds(pl.multiple_of(e * cap, cap), cap)] = send_stage[0]
    lax.fori_loop(0, first_cut, weight_step, 0)
    for load in late[3:]:
        load.wait()
    first, second = [
        expert_lane == jnp.transpose(jnp.broadcast_to(ids[j : j + 1], (128, tokens)))[:, 0:1]
        for j, expert_lane in enumerate(
            [lax.broadcasted_iota(jnp.int32, (tokens, experts), 1)] * 2
        )
    ]
    expert_lane = lax.broadcasted_iota(jnp.int32, (tokens, experts), 1)
    order = dot((row > col).astype(f32), (first | second).astype(f32)).astype(jnp.int32)
    spots = expert_lane * cap + order
    slot_lane = lax.broadcasted_iota(jnp.int32, (tokens, experts * cap), 1)
    first_slot = jnp.sum(jnp.where(first, spots, 0), axis=1, keepdims=True)
    second_slot = jnp.sum(jnp.where(second, spots, 0), axis=1, keepdims=True)
    pick = ((slot_lane == first_slot) | (slot_lane == second_slot)).astype(f32).astype(bf16)

    def came_back(k, carry):
        source = flip(k)
        spot = returned.at[pl.ds(pl.multiple_of(source * cap, cap), cap)]
        remote(spot, spot, back_send.at[k], back_recv.at[k], (source, p, t)).wait_recv()
        return carry

    lax.fori_loop(1, experts, came_back, 0)
    moe = lax.dot_general(pick, returned[...], PLAIN, preferred_element_type=f32)
    mid_half = (out_grad[:, own_columns].astype(f32) + moe).astype(bf16)
    mid[:, own_columns] = mid_half

    def to_core(columns):
        return remote(mid.at[:, columns], mid.at[:, columns], mid_send, mid_recv, mate_id)

    to_core(own_columns).start()
    share = count // 2
    piece = width // share
    for j in range(share):
        mid_stage[j] = mid_half[:, j * piece : (j + 1) * piece]
    position = position_ref[...]
    q_all = queries[...].astype(f32)
    k_all = keys[...].astype(f32)
    v_all = values[...]
    cumul = [position[:BLK]]
    for n in range(1, blocks):
        cumul.append(position[n * BLK : (n + 1) * BLK] - position[n * BLK - 1 : n * BLK])
    growth = [jnp.exp(c) for c in cumul]
    shrink = [jnp.exp(-c) for c in cumul]
    to_end = [jnp.exp(c[BLK - 1 :] - c) for c in cumul]
    span = [slice(n * BLK, (n + 1) * BLK) for n in range(blocks)]
    q_grow = [(q_all[span[n]] * growth[n]).astype(bf16) for n in range(blocks)]
    k_shrink = [(k_all[span[n]] * shrink[n]).astype(bf16) for n in range(blocks)]
    k_end = [(k_all[span[n]] * to_end[n]).astype(bf16) for n in range(blocks)]
    q_long = (q_all * jnp.exp(position)).astype(bf16)

    to_core(core_columns).wait_recv()
    o_all = dot(mid[...], out_weight[...], ACROSS).astype(bf16)
    for h in range(heads):
        ks, vs = slice(h * DK, (h + 1) * DK), slice(h * DV, (h + 1) * DV)
        summed = dot(q_long[:, ks], o_all[:, vs], DOWNWARD)
        for j in range(per_head):
            sum_stage[h * per_head + j] = summed[j * rows : (j + 1) * rows]
    sum_held[me] = sum_stage[me]
    for k in range(1, count):
        spread(lambda i: sum_stage.at[i], sum_held.at[me], sum_send, sum_recv, k).start()

    direct_half = lax.div(e, half_experts) == t

    def column_copies(act):
        for a in range(half_experts // 2):
            for q in range(2):
                dest_e = t * half_experts + 2 * a + low
                for w in range(2):
                    column = (2 * a + (low if w == 0 else 1 - low)) * 2 + q

                    @pl.when(jnp.logical_or(dest_e != e, q != p))
                    def _():
                        act(
                            remote(
                                mid_stage.at[column], mid_columns.at[w, here],
                                col_send.at[w, a * 2 + q], col_recv.at[w, here], (dest_e, q, t),
                            )
                        )

    column_copies(lambda copy: copy.start())

    @pl.when(direct_half)
    def _():
        base = lax.rem(e, half_experts) - low
        mid_columns[0, here] = mid_stage[(base + low) * 2 + p]
        mid_columns[1, here] = mid_stage[(base + 1 - low) * 2 + p]

    lane_causal = row[:BLK, :BLK] >= col[:BLK, :BLK]
    lane_causal_t = row[:BLK, :BLK] <= col[:BLK, :BLK]
    for n in range(blocks - 1, -1, -1):
        for h in range(heads):
            ks, vs = slice(h * DK, (h + 1) * DK), slice(h * DV, (h + 1) * DV)
            o, v = o_all[span[n], vs], v_all[span[n], vs]
            qg, kk = q_grow[n][:, ks], k_shrink[n][:, ks]
            state_in = block_states[n, h].astype(bf16)
            scores = jnp.where(lane_causal, dot(o, v, ACROSS), 0.0)
            scores_t = jnp.where(lane_causal_t, dot(v, o, ACROSS), 0.0)
            mutual_t = jnp.where(lane_causal_t, dot(kk, qg, ACROSS), 0.0)
            gq = growth[n][:, ks] * (dot(o, state_in, ACROSS) + dot(scores, kk))
            gk = shrink[n][:, ks] * dot(scores_t, qg)
            gv = dot(mutual_t, o)
            if n < blocks - 1:
                later = slice((n + 1) * BLK, tokens)
                end = position[(n + 1) * BLK - 1 : (n + 1) * BLK, ks]
                carried = dot(
                    q_all[later, ks] * jnp.exp(position[later, ks] - end), o_all[later, vs], DOWNWARD
                )
                gk = gk + to_end[n][:, ks] * dot(v, carried, ACROSS)
                gv = gv + dot(k_end[n][:, ks], carried)
            grad_q[span[n], ks] = gq
            key_local[span[n], ks] = gk
            value_local[span[n], vs] = gv
    contrib = q_all * grad_q[...] - k_all * key_local[...]
    contrib_local[...] = contrib
    gathered[me] = jnp.sum(contrib, axis=0, keepdims=True)
    for k in range(1, count):
        spread(lambda i: gathered.at[me], gathered.at[me], term_send, term_recv, k).start()

    lax.fori_loop(first_cut, second_cut, weight_step, 0)
    for k in range(1, count):
        landed(early_held, early_send, early_recv, k)
        landed(sum_held, sum_send, sum_recv, k)
    total = jnp.zeros((rows, DV), f32)
    dots = jnp.zeros((rows, DV), f32)
    for i in range(count - 1, -1, -1):
        result[i] = total
        dot_result[i] = dots
        reach_dot = jnp.sum(early_held[i, 0] * total, axis=1, keepdims=True)
        dots = dots + jnp.broadcast_to(reach_dot, (rows, DV))
        total = early_held[i, 1] * total + sum_held[i]
    from_right[me] = result[me]
    decay_dots[me] = dot_result[me]
    def right_copy(k):
        return spread(lambda i: result.at[i], from_right.at[me], right_send, right_recv, k)

    def dot_copy(k):
        return spread(lambda i: dot_result.at[i], decay_dots.at[me], dot_send, dot_recv, k)

    for k in range(1, count):
        right_copy(k).start()
        dot_copy(k).start()

    def cross_copy():
        return remote(mid_columns, mid_columns, cross_send, cross_recv, mate_id)

    @pl.when(direct_half)
    def _():
        for k in range(1, share):
            source = lax.rem(here + k, share)
            for w in range(2):
                spot = mid_columns.at[w, source]
                remote(
                    spot, spot, col_send.at[w, 0], col_recv.at[w, source], mate_id
                ).wait_recv()
        cross_copy().start()

    lax.fori_loop(second_cut, weight_steps, weight_step, 0)

    @pl.when(jnp.logical_not(direct_half))
    def _():
        cross_copy().wait_recv()

    for k in range(half_experts):
        mixer_side(k, 1 - p).wait_recv()
    for w in (1, 0):
        product = dot(
            mid_columns[w].reshape(share * tokens, piece),
            mixers[...].reshape(share * tokens, mixers.shape[2]),
            DOWNWARD,
        )
        if w:
            near_part[...] = product
            near = remote(near_part, near_held, near_send, near_recv, (flip(1), p, t))
            near.start()
        else:
            grad_out[...] = product
    near.wait_recv()
    grad_out[...] = grad_out[...] + near_held[...]
    for k in range(1, count):
        landed(gathered, term_send, term_recv, k)
    summed_terms = jnp.zeros((1, channels), f32)
    for i in range(count):
        summed_terms += jnp.where(i > me, gathered[i], 0.0)
    right_terms[...] = summed_terms
    for k in range(1, count):
        landed(from_right, right_send, right_recv, k)
        landed(decay_dots, dot_send, dot_recv, k)
    to_core(own_columns).wait_send()
    near.wait_send()
    column_copies(lambda copy: copy.wait_send())

    @pl.when(direct_half)
    def _():
        cross_copy().wait_send()

    for k in range(1, count):
        early_copy(k).wait_send()
        spread(lambda i: sum_stage.at[i], sum_held.at[me], sum_send, sum_recv, k).wait_send()
        right_copy(k).wait_send()
        dot_copy(k).wait_send()
        spread(lambda i: gathered.at[me], gathered.at[me], term_send, term_recv, k).wait_send()

    def close(k, carry):
        for a in range(2):
            to_pair(a, k, p).wait_send()
            to_mate(a, k, p, 0, own_columns).wait_send()
            to_mate(a, k, 1 - p, 1, own_columns).wait_send()
        core_copy(0, k).wait_send()
        core_copy(1, k).wait_send()
        pair_copy(k).wait_send()

        @pl.when(k > 0)
        def _():
            direct(0, k).wait_send()
            direct(1, k).wait_send()
            back_copy(k).wait_send()

        return carry

    lax.fori_loop(0, experts, close, 0)
    for k in range(half_experts):
        if k:
            mixer_copy(k).wait_send()
        mixer_side(k, p).wait_send()
    pltpu.make_async_copy(down_stage, down_out, out_sem.at[0]).wait()
    pltpu.make_async_copy(gate_stage, gate_out, out_sem.at[1]).wait()
    pltpu.make_async_copy(up_stage, up_out, out_sem.at[2]).wait()


def layer_back(
    cap, ids, route_weights, moe_input, out_grad, gate_w, up_w, down_w, mixer, out_weight,
    queries, keys, values, log_decay, block_states,
):
    experts = lax.axis_size("ep")
    count = experts * 2
    tokens, model_width = moe_input.shape
    units = gate_w.shape[1]
    width = model_width // lax.axis_size("tp")
    slots = experts * 2 * cap
    channels = queries.shape[1]
    rows = channels // count
    share = count // 2
    piece = width // share
    half = (experts, cap, width)
    vmem = pl.BlockSpec(memory_space=pltpu.VMEM)
    hbm = pl.BlockSpec(memory_space=pltpu.HBM)
    dma = pltpu.SemaphoreType.DMA
    wide, tall = (model_width, units), (units, model_width)
    kind, f32 = jnp.bfloat16, jnp.float32
    shape = jax.ShapeDtypeStruct
    group_rows = PER_GROUP * 2 * cap
    local = shape((tokens, channels), f32)
    exchanged = shape((count, rows, DV), f32)
    keep = pltpu.VMEM
    return pl.pallas_call(
        functools.partial(experts_kernel, experts, cap),
        out_shape=(
            shape(wide, kind),
            shape(wide, kind),
            shape(tall, kind),
            shape((piece, mixer.shape[1]), f32),
            exchanged,
            exchanged,
            shape((1, channels), f32),
            local,
            local,
            shape(values.shape, f32),
            local,
            local,
            local,
        ),
        in_specs=[vmem] * 4 + [hbm] * 10,
        out_specs=(hbm,) * 3 + (vmem,) * 10,
        scratch_shapes=[
            keep(out_weight.shape, kind),
            keep(queries.shape, kind),
            keep(keys.shape, kind),
            keep(values.shape, kind),
            keep(log_decay.shape, f32),
            keep(block_states.shape, f32),
            keep((share,) + mixer.shape, kind),
            keep((experts * cap, width), kind),
            keep((tokens, channels), f32),
            keep((tokens, model_width), kind),
            keep((share, tokens, piece), kind),
            keep((2, share, tokens, piece), kind),
            keep((count, 2, rows, DV), f32),
            keep((count, 2, rows, DV), f32),
            keep((count, rows, DV), f32),
            keep((count, rows, DV), f32),
            keep((count, rows, DV), f32),
            keep((count, rows, DV), f32),
            keep((count, 1, channels), f32),
            keep((piece, mixer.shape[1]), f32),
            keep((piece, mixer.shape[1]), f32),
            keep((slots, model_width), kind),
            keep((slots, model_width), kind),
            keep((slots, units), kind),
            keep((slots, 2 * units), kind),
            keep((model_width, 2 * units), kind),
            keep(tall, kind),
            keep((group_rows, units), f32),
            keep((group_rows, units), f32),
            keep((slots, model_width), kind),
            keep((experts, tokens), jnp.int32),
            keep(half, kind),
            keep(half, kind),
            keep((2,) + half, kind),
            keep(half, kind),
            keep(half, kind),
            keep(half, kind),
            keep(wide, kind),
            keep(wide, kind),
            keep(tall, kind),
            dma((3,)),
            dma((3,)),
            *(dma((2, experts)) for _ in range(4)),
            *(dma((2, 2, experts)) for _ in range(2)),
            *(dma((2, experts)) for _ in range(2)),
            *(dma((experts,)) for _ in range(4)),
            dma((7,)),
            *(dma((experts // 2,)) for _ in range(4)),
            dma,
            dma,
            dma((2, share)),
            dma((2, share)),
            *(dma for _ in range(4)),
            *(dma((count,)) for _ in range(10)),
        ],
        compiler_params=pltpu.CompilerParams(
            collective_id=0, has_side_effects=True, vmem_limit_bytes=62 * 1024 * 1024
        ),
        name="layer_back",
    )(
        ids, route_weights, moe_input, out_grad, gate_w, up_w, down_w, mixer, out_weight, queries,
        keys, values, log_decay, block_states,
    )


def finish_kernel(
    chunks, grad_out_turned, from_right, decay_dots, right_terms, query_local, key_local,
    value_local, contrib_local, k_fade, fade_out, values, weight_a, weight_b, weight_c,
    grad_q, grad_k, grad_v, grad_decay, grad_out, out_a, out_b, out_c,
    hold_a, hold_b, hold_c, in_sem, out_sem,
):
    f32, bf16 = jnp.float32, jnp.bfloat16
    trios = ((weight_a, hold_a, out_a), (weight_b, hold_b, out_b), (weight_c, hold_c, out_c))

    def moves(a, j):
        source, hold, target = trios[a]
        size = source.shape[0] // chunks
        cut = pl.ds(j * size, size)
        return (
            pltpu.make_async_copy(source.at[cut], hold.at[cut], in_sem.at[a, j]),
            pltpu.make_async_copy(hold.at[cut], target.at[cut], out_sem.at[a, j]),
        )

    steps = [(a, j) for a in range(3) for j in range(chunks)]
    for a, j in steps:
        moves(a, j)[0].start()

    def dot(x, y, dims=(((1,), (0,)), ((), ()))):
        return lax.dot_general(
            x.astype(bf16), y.astype(bf16), dims, preferred_element_type=f32
        )

    def forward(group):
        for a, j in group:
            moves(a, j)[0].wait()
            moves(a, j)[1].start()

    tokens, channels = key_local.shape
    heads = channels // DK
    grad_q[...] = query_local[...].astype(bf16)
    forward(steps[:chunks])
    key_parts = []
    for h in range(heads):
        ks, vs = slice(h * DK, (h + 1) * DK), slice(h * DV, (h + 1) * DV)
        carried = from_right[h].astype(bf16)
        key_parts.append(dot(values[:, vs], carried, ACROSS))
        grad_v[:, vs] = (value_local[:, vs] + dot(k_fade[:, ks], carried)).astype(bf16)
    key_part = jnp.concatenate(key_parts, axis=1)
    grad_k[...] = (key_local[...] + fade_out[...] * key_part).astype(bf16)
    contrib = contrib_local[...] - k_fade[...] * key_part
    forward(steps[chunks : 2 * chunks])
    row = lax.broadcasted_iota(jnp.int32, (tokens, tokens), 0)
    col = lax.broadcasted_iota(jnp.int32, (tokens, tokens), 1)
    later = (col >= row).astype(f32)
    groups = []
    spot = lax.broadcasted_iota(jnp.int32, (128, 128), 0)
    lane = lax.broadcasted_iota(jnp.int32, (128, 128), 1)
    for g in range(channels // 128):
        picked = jnp.where(spot == lane, decay_dots[g * 128 : (g + 1) * 128], 0.0)
        groups.append(jnp.sum(picked, axis=0, keepdims=True))
    right = right_terms[...] - jnp.concatenate(groups, axis=1)
    grad_decay[...] = right + lax.dot_general(
        later, contrib, (((1,), (0,)), ((), ())), precision=PRECISE, preferred_element_type=f32
    )
    grad_out[...] = jnp.transpose(grad_out_turned[...])
    forward(steps[2 * chunks :])
    for a, j in steps:
        moves(a, j)[1].wait()


def finish(local, values, weights):
    grad_out_turned, from_right, decay_dots, right_terms, *rest = local
    tokens, channels = rest[1].shape
    heads = channels // DK
    from_right = from_right.reshape(heads, DK, DV)
    decay_dots = decay_dots.reshape(channels, DV)
    vmem = pl.BlockSpec(memory_space=pltpu.VMEM)
    hbm = pl.BlockSpec(memory_space=pltpu.HBM)
    dma = pltpu.SemaphoreType.DMA
    shape = jax.ShapeDtypeStruct
    f32, bf16 = jnp.float32, jnp.bfloat16
    chunks = 4
    return pl.pallas_call(
        functools.partial(finish_kernel, chunks),
        out_shape=(
            shape((tokens, channels), bf16),
            shape((tokens, channels), bf16),
            shape((tokens, heads * DV), bf16),
            shape((tokens, channels), f32),
            shape(grad_out_turned.shape[::-1], f32),
            *(shape(w.shape, w.dtype) for w in weights),
        ),
        in_specs=[vmem] * 11 + [hbm] * 3,
        out_specs=(vmem,) * 5 + (hbm,) * 3,
        scratch_shapes=[pltpu.VMEM(w.shape, w.dtype) for w in weights]
        + [dma((3, chunks)), dma((3, chunks))],
        compiler_params=pltpu.CompilerParams(vmem_limit_bytes=60 * 1024 * 1024),
        name="finish",
    )(grad_out_turned, from_right, decay_dots, right_terms, *rest, values, *weights)


def body(
    moe_input,
    out_grad,
    route_ids,
    route_weights,
    gate_w,
    up_w,
    down_w,
    mixer_out,
    out_weight,
    queries,
    keys,
    values,
    log_decay,
    block_states,
):
    experts = lax.axis_size("ep")
    cap = -(-3 * moe_input.shape[0] // experts // 16) * 16
    results = layer_back(
        cap, route_ids.T, route_weights.T, moe_input, out_grad, gate_w[0], up_w[0], down_w[0],
        mixer_out, out_weight, queries, keys, values, log_decay, block_states,
    )
    weights, local = results[:3], results[3:]
    grad_q, grad_k, grad_v, grad_decay, grad_out_weight, grad_gate, grad_up, grad_down = finish(
        local, values, weights
    )
    return (
        grad_q,
        grad_k,
        grad_v,
        grad_decay,
        grad_out_weight,
        grad_gate[None],
        grad_up[None],
        grad_down[None],
    )


def solution(mesh):
    sp_count, tp_count = mesh.devices.shape
    mesh = Mesh(mesh.devices.reshape(sp_count // 2, 2, tp_count), ("ep", "pair", "tp"))
    placed = (
        P(SP, None),
        P(SP, None),
        P(SP, None),
        P(SP, None),
        P(SP, None, "tp"),
        P(SP, None, "tp"),
        P(SP, "tp", None),
        P(SP, "tp"),
        P("tp", None),
        P(SP, "tp"),
        P(SP, "tp"),
        P(SP, "tp"),
        P(SP, "tp"),
        P(SP, "tp", None, None),
    )
    return jax.shard_map(
        body,
        mesh=mesh,
        in_specs=placed,
        out_specs=(
            P(SP, "tp"),
            P(SP, "tp"),
            P(SP, "tp"),
            P(SP, "tp"),
            P("tp", SP),
            P(SP, None, "tp"),
            P(SP, None, "tp"),
            P(SP, "tp", None),
        ),
        check_vma=False,
    )
```

```python
import functools

import jax
import jax.numpy as jnp
from jax import lax
from jax.experimental import pallas as pl
from jax.experimental.pallas import tpu as pltpu
from jax.sharding import Mesh, PartitionSpec as P

MESH = pl.DeviceIdType.MESH
SP = ("ep", "pair")

DK = 64
DV = 128
BLK = 64
PER_GROUP = 2


PRECISE = lax.Precision.HIGHEST
ACROSS = (((1,), (1,)), ((), ()))
DOWNWARD = (((0,), (0,)), ((), ()))
PLAIN = (((1,), (0,)), ((), ()))


def sp_size():
    return lax.axis_size("ep") * lax.axis_size("pair")


def sp_index():
    return lax.axis_index("ep") * lax.axis_size("pair") + lax.axis_index("pair")


def experts_kernel(
    experts, cap, ids, route_weights, moe_input, out_grad, gate_w, up_w, down_w,
    mixer_hbm, out_weight_hbm, queries_hbm, keys_hbm, values_hbm, log_decay_hbm, block_states_hbm,
    gate_out, up_out, down_out, grad_out, from_right, decay_dots, right_terms, grad_q, key_local,
    value_local, contrib_local, k_fade, fade_out,
    out_weight, queries, keys, values, log_decay, block_states, mixers, returned, position_ref,
    mid, mid_stage, mid_columns, early_stage, early_held, sum_stage, sum_held, result, dot_result,
    gathered, gains, near_part, near_held,
    toks, grads, hidden, d_both, gate_up, down, silu_part, slope_part, parts, rank, tok_send,
    grad_send, core_held, pair_held,
    weight_sem, direct_send, direct_recv, pass_send, pass_recv, mate_send, mate_recv,
    core_send, core_recv, pair_send, pair_recv, back_send, back_recv,
    load_sem, mixer_send, mixer_recv, side_send, side_recv, mid_send, mid_recv, col_send, col_recv,
    cross_send, cross_recv, near_send, near_recv, early_send, early_recv, sum_send, sum_recv,
    right_send, right_recv, dot_send, dot_recv, term_send, term_recv, gain_send, gain_recv,
):
    e, p, t = lax.axis_index("ep"), lax.axis_index("pair"), lax.axis_index("tp")
    f32, bf16 = jnp.float32, jnp.bfloat16
    tokens, model_width = moe_input.shape
    width = model_width // 2
    units = hidden.shape[1]
    group_rows = PER_GROUP * 2 * cap
    groups = experts // PER_GROUP
    pair_id, mate_id = (e, 1 - p, t), (e, p, 1 - t)
    barrier = pltpu.get_barrier_semaphore()
    me = e * 2 + p
    count = experts * 2
    half_experts = experts // 2
    low, high = lax.rem(e, 2), lax.div(e, 2)
    here = high * 2 + p

    def place(i):
        return (lax.div(i, 2), lax.rem(i, 2), t)

    for k in range(1, count):
        pl.semaphore_signal(
            barrier, inc=1, device_id=place(lax.rem(me + k, count)), device_id_type=MESH
        )
    pl.semaphore_signal(barrier, inc=1, device_id=mate_id, device_id_type=MESH)

    def flip(k):
        total, bit = 0, 1
        while bit < experts:
            other = k // bit if isinstance(k, int) else lax.div(k, bit)
            total = total + bit * lax.rem(lax.div(e, bit) + other, 2)
            bit *= 2
        return total

    own_mixer = pltpu.make_async_copy(mixer_hbm, mixers.at[here], load_sem.at[6])
    late = [
        pltpu.make_async_copy(src, dst, load_sem.at[i])
        for i, (src, dst) in enumerate(
            (
                (log_decay_hbm, log_decay),
                (keys_hbm, keys),
                (values_hbm, values),
                (queries_hbm, queries),
                (out_weight_hbm, out_weight),
                (block_states_hbm, block_states),
            )
        )
    ]
    loads = (
        pltpu.make_async_copy(gate_w, gate_up.at[:, pl.ds(0, units)], weight_sem.at[0]),
        pltpu.make_async_copy(up_w, gate_up.at[:, pl.ds(units, units)], weight_sem.at[1]),
        pltpu.make_async_copy(down_w, down, weight_sem.at[2]),
    )
    for load in late[:3] + list(loads) + late[3:] + [own_mixer]:
        load.start()
    own_columns = pl.ds(pl.multiple_of(t * width, 128), width)
    core_columns = pl.ds(pl.multiple_of((1 - t) * width, 128), width)
    arrived = (toks, grads)
    sends = (tok_send, grad_send)

    def block(k, side):
        return pl.ds(pl.multiple_of((k * 2 + side) * cap, cap), cap)

    def remote(src, dst, send, recv, device):
        return pltpu.make_async_remote_copy(
            src_ref=src, dst_ref=dst, send_sem=send, recv_sem=recv, device_id=device,
            device_id_type=MESH,
        )

    def direct(a, k):
        return remote(
            sends[a].at[k], arrived[a].at[block(k, p), own_columns], direct_send.at[a, k],
            direct_recv.at[a, k], (flip(k), p, t),
        )

    def to_pair(a, k, side):
        place = arrived[a].at[block(k, side), own_columns]
        return remote(place, place, pass_send.at[a, k], pass_recv.at[a, k], pair_id)

    def to_mate(a, k, side, which, columns):
        place = arrived[a].at[block(k, side), columns]
        return remote(place, place, mate_send.at[a, which, k], mate_recv.at[a, which, k], mate_id)

    first_id, second_id = ids[0:1], ids[1:2]
    first_w, second_w = route_weights[0:1], route_weights[1:2]
    expert_row = lax.broadcasted_iota(jnp.int32, (experts, tokens), 0)
    member = (expert_row == first_id) | (expert_row == second_id)
    row = lax.broadcasted_iota(jnp.int32, (tokens, tokens), 0)
    col = lax.broadcasted_iota(jnp.int32, (tokens, tokens), 1)
    before = (row < col).astype(bf16)
    earlier = lax.dot_general(
        member.astype(f32).astype(bf16), before, PLAIN, preferred_element_type=f32
    )
    rank[...] = jnp.where(member, earlier.astype(jnp.int32), -1)
    spot = lax.broadcasted_iota(jnp.int32, (cap, tokens), 0)

    def rows_for(dest):
        pick = spot == rank[pl.ds(dest, 1)]
        weight = jnp.where(first_id == dest, first_w, second_w)
        scale = jnp.sum(jnp.where(pick, weight, 0.0), axis=1, keepdims=True)
        chosen = pick.astype(f32).astype(bf16)
        tok = lax.dot_general(chosen, moe_input[:, own_columns], PLAIN, preferred_element_type=f32)
        grad = lax.dot_general(chosen, out_grad[:, own_columns], PLAIN, preferred_element_type=f32)
        return tok.astype(bf16), (scale * grad).astype(bf16)

    own_tok, own_grad = rows_for(e)
    toks[block(0, p), own_columns] = own_tok
    grads[block(0, p), own_columns] = own_grad
    pl.semaphore_wait(barrier, count)
    for a in range(2):
        to_pair(a, 0, p).start()
        to_mate(a, 0, p, 0, own_columns).start()

    def send_step(k, carry):
        tok, grad = rows_for(flip(k))
        tok_send[k] = tok
        grad_send[k] = grad
        direct(0, k).start()
        direct(1, k).start()
        return carry

    lax.fori_loop(1, experts, send_step, 0)

    def mixer_copy(k):
        dest = lax.rem(high + k, half_experts) * 2 + low
        return remote(
            mixer_hbm, mixers.at[here], mixer_send.at[k], mixer_recv.at[k], (dest, p, t)
        )

    def mixer_place(k, side):
        return mixers.at[lax.rem(high - k + half_experts, half_experts) * 2 + side]

    def mixer_landed(k):
        spot = mixer_place(k, p)
        remote(spot, spot, mixer_send.at[k], mixer_recv.at[k], pair_id).wait_recv()

    def mixer_side(k, side):
        spot = mixer_place(k, side)
        return remote(spot, spot, side_send.at[k], side_recv.at[k], pair_id)

    for k in range(1, half_experts):
        mixer_copy(k).start()

    channels = queries.shape[1]
    heads = channels // DK
    blocks = tokens // BLK
    rows = channels // count
    per_head = DK // rows

    def dot(x, y, dims=PLAIN):
        return lax.dot_general(
            x.astype(bf16), y.astype(bf16), dims, preferred_element_type=f32
        )

    def spread(src, dst, sends, recvs, k):
        dest = lax.rem(me + k, count)
        return remote(src(dest), dst, sends.at[k], recvs.at[k], place(dest))

    def landed(ref, sends, recvs, k):
        source = lax.rem(me - k + count, count)
        remote(ref.at[source], ref.at[source], sends.at[k], recvs.at[k], place(source)).wait_recv()

    def early_copy(k):
        return spread(lambda i: early_stage.at[i], early_held.at[me], early_send, early_recv, k)

    for load in late[:3]:
        load.wait()
    position_ref[...] = lax.dot_general(
        (row >= col).astype(f32), log_decay[...], PLAIN, precision=PRECISE,
        preferred_element_type=f32,
    )
    device_total = position_ref[tokens - 1 :]
    fade = jnp.exp(device_total - position_ref[...])
    faded = keys[...].astype(f32) * fade
    fade_out[...] = fade
    k_fade[...] = faded
    gains[me] = jnp.exp(device_total)
    for h in range(heads):
        ks, vs = slice(h * DK, (h + 1) * DK), slice(h * DV, (h + 1) * DV)
        reach = dot(faded[:, ks], values[:, vs], DOWNWARD)
        for j in range(per_head):
            early_stage[h * per_head + j] = reach[j * rows : (j + 1) * rows].astype(bf16)
    early_held[me] = early_stage[me]

    def gain_copy(k):
        return spread(lambda i: gains.at[me], gains.at[me], gain_send, gain_recv, k)

    for k in range(1, count):
        early_copy(k).start()
        gain_copy(k).start()
    for load in loads:
        load.wait()

    def from_direct(a, k):
        @pl.when(k > 0)
        def _():
            direct(a, k).wait_recv()
            to_pair(a, k, p).start()
            to_mate(a, k, p, 0, own_columns).start()

    def from_pair(a, k):
        to_pair(a, k, 1 - p).wait_recv()
        to_mate(a, k, 1 - p, 1, own_columns).start()

    def from_mate(a, k):
        to_mate(a, k, p, 0, core_columns).wait_recv()
        to_mate(a, k, 1 - p, 1, core_columns).wait_recv()

    def core_copy(which, k):
        side = 1 - p if which == 0 else p
        return remote(
            parts.at[block(k, side), core_columns], core_held.at[which, k],
            core_send.at[which, k], core_recv.at[which, k], mate_id,
        )

    def pair_copy(k):
        return remote(
            parts.at[block(k, 1 - p), own_columns], pair_held.at[k], pair_send.at[k], pair_recv.at[k], pair_id
        )

    def back_copy(k):
        return remote(
            parts.at[block(k, p), own_columns], returned.at[pl.ds(pl.multiple_of(e * cap, cap), cap)], back_send.at[k], back_recv.at[k], (flip(k), p, t)
        )

    def half_of(which, k):
        side = 1 - p if which == 0 else p
        mine = parts[block(k, side), own_columns].astype(f32)
        return (mine + core_held[which, k].astype(f32)).astype(bf16)

    def members(g):
        return [g * PER_GROUP + j for j in range(PER_GROUP)]

    def half_step(g):
        for k in members(g):
            core_copy(0, k).wait_recv()
            parts[block(k, 1 - p), own_columns] = half_of(0, k)
            pair_copy(k).start()

    def total_step(g):
        for k in members(g):
            core_copy(1, k).wait_recv()
            pair_copy(k).wait_recv()
            total = half_of(1, k).astype(f32) + pair_held[k].astype(f32)
            parts[block(k, p), own_columns] = total.astype(bf16)

            @pl.when(k > 0)
            def _():
                back_copy(k).start()

    def group_step(g, carry):
        now, last = members(g), members(g - 1)
        rows = pl.ds(pl.multiple_of((g - 1) * group_rows, group_rows), group_rows)
        coming, behind = g < groups, g > 0

        @pl.when(coming)
        def _():
            for k in now:
                from_direct(0, k)

        @pl.when(behind)
        def _():
            for k in last:
                from_mate(0, k)
            gate_pre = lax.dot_general(
                toks[rows], gate_up[:, :units], PLAIN, preferred_element_type=f32
            )
            gate = jax.nn.sigmoid(gate_pre)
            silu_part[...] = gate_pre * gate
            slope_part[...] = gate * (1.0 + gate_pre * (1.0 - gate))

        @pl.when(coming)
        def _():
            for k in now:
                from_direct(1, k)
                from_pair(0, k)

        @pl.when(behind)
        def _():
            up_pre = lax.dot_general(
                toks[rows], gate_up[:, units:], PLAIN, preferred_element_type=f32
            )
            hidden[rows] = (silu_part[...] * up_pre).astype(bf16)
            slope_part[...] = slope_part[...] * up_pre
            for k in last:
                from_mate(1, k)

        @pl.when(coming)
        def _():
            for k in now:
                from_pair(1, k)

        @pl.when(behind)
        def _():
            d_hidden = lax.dot_general(grads[rows], down[...], ACROSS, preferred_element_type=f32)
            d_both[rows, :units] = (d_hidden * slope_part[...]).astype(bf16)
            d_both[rows, units:] = (d_hidden * silu_part[...]).astype(bf16)
            parts[rows, core_columns] = lax.dot_general(
                d_both[rows], gate_up[core_columns], ACROSS, preferred_element_type=f32
            ).astype(bf16)
            for k in last:
                core_copy(0, k).start()
                core_copy(1, k).start()

        @pl.when(g > 1)
        def _():
            total_step(g - 2)

        @pl.when(behind)
        def _():
            parts[rows, own_columns] = lax.dot_general(
                d_both[rows], gate_up[own_columns], ACROSS, preferred_element_type=f32
            ).astype(bf16)
            half_step(g - 1)

        return carry

    lax.fori_loop(0, groups + 1, group_step, 0)

    def down_step(i, carry):
        cut = pl.ds(pl.multiple_of(i * 128, 128), 128)
        down_out[cut, :] = lax.dot_general(
            hidden[:, cut], grads[...], DOWNWARD, preferred_element_type=f32
        ).astype(bf16)
        return carry

    def weight_step(i, carry):
        cut = pl.ds(pl.multiple_of(i * 256, 256), 256)
        both = lax.dot_general(
            toks[:, cut], d_both[...], DOWNWARD, preferred_element_type=f32
        ).astype(bf16)
        gate_out[cut, :] = both[:, :units]
        up_out[cut, :] = both[:, units:]
        return carry

    weight_steps = model_width // 256
    first_cut, second_cut = weight_steps // 4, weight_steps // 2
    own_mixer.wait()
    mixer_side(0, p).start()
    for k in range(1, half_experts):
        mixer_landed(k)
        mixer_side(k, p).start()
    lax.fori_loop(0, units // 128, down_step, 0)
    total_step(groups - 1)
    returned[pl.ds(pl.multiple_of(e * cap, cap), cap)] = parts[
        block(0, p), own_columns
    ]
    lax.fori_loop(0, first_cut, weight_step, 0)
    for load in late[3:]:
        load.wait()
    first, second = [
        expert_lane == jnp.transpose(jnp.broadcast_to(ids[j : j + 1], (128, tokens)))[:, 0:1]
        for j, expert_lane in enumerate(
            [lax.broadcasted_iota(jnp.int32, (tokens, experts), 1)] * 2
        )
    ]
    expert_lane = lax.broadcasted_iota(jnp.int32, (tokens, experts), 1)
    order = dot((row > col).astype(f32), (first | second).astype(f32)).astype(jnp.int32)
    spots = expert_lane * cap + order
    slot_lane = lax.broadcasted_iota(jnp.int32, (tokens, experts * cap), 1)
    first_slot = jnp.sum(jnp.where(first, spots, 0), axis=1, keepdims=True)
    second_slot = jnp.sum(jnp.where(second, spots, 0), axis=1, keepdims=True)
    pick = ((slot_lane == first_slot) | (slot_lane == second_slot)).astype(f32).astype(bf16)

    def came_back(k, carry):
        source = flip(k)
        spot = returned.at[pl.ds(pl.multiple_of(source * cap, cap), cap)]
        remote(spot, spot, back_send.at[k], back_recv.at[k], (source, p, t)).wait_recv()
        return carry

    lax.fori_loop(1, experts, came_back, 0)
    moe = lax.dot_general(pick, returned[...], PLAIN, preferred_element_type=f32)
    mid_half = (out_grad[:, own_columns].astype(f32) + moe).astype(bf16)
    mid[:, own_columns] = mid_half

    def to_core(columns):
        return remote(mid.at[:, columns], mid.at[:, columns], mid_send, mid_recv, mate_id)

    to_core(own_columns).start()
    share = count // 2
    piece = width // share
    for j in range(share):
        mid_stage[j] = mid_half[:, j * piece : (j + 1) * piece]
    position = position_ref[...]
    q_all = queries[...].astype(f32)
    k_all = keys[...].astype(f32)
    v_all = values[...]
    cumul = [position[:BLK]]
    for n in range(1, blocks):
        cumul.append(position[n * BLK : (n + 1) * BLK] - position[n * BLK - 1 : n * BLK])
    growth = [jnp.exp(c) for c in cumul]
    shrink = [jnp.exp(-c) for c in cumul]
    to_end = [jnp.exp(c[BLK - 1 :] - c) for c in cumul]
    span = [slice(n * BLK, (n + 1) * BLK) for n in range(blocks)]
    q_grow = [(q_all[span[n]] * growth[n]).astype(bf16) for n in range(blocks)]
    k_shrink = [(k_all[span[n]] * shrink[n]).astype(bf16) for n in range(blocks)]
    k_end = [(k_all[span[n]] * to_end[n]).astype(bf16) for n in range(blocks)]
    q_long = (q_all * jnp.exp(position)).astype(bf16)

    to_core(core_columns).wait_recv()
    o_all = dot(mid[...], out_weight[...], ACROSS).astype(bf16)
    for h in range(heads):
        ks, vs = slice(h * DK, (h + 1) * DK), slice(h * DV, (h + 1) * DV)
        summed = dot(q_long[:, ks], o_all[:, vs], DOWNWARD)
        for j in range(per_head):
            sum_stage[h * per_head + j] = summed[j * rows : (j + 1) * rows].astype(bf16)
    sum_held[me] = sum_stage[me]
    for k in range(1, count):
        spread(lambda i: sum_stage.at[i], sum_held.at[me], sum_send, sum_recv, k).start()

    direct_half = lax.div(e, half_experts) == t

    def column_copies(act):
        for a in range(half_experts // 2):
            for q in range(2):
                dest_e = t * half_experts + 2 * a + low
                for w in range(2):
                    column = (2 * a + (low if w == 0 else 1 - low)) * 2 + q

                    @pl.when(jnp.logical_or(dest_e != e, q != p))
                    def _():
                        act(
                            remote(
                                mid_stage.at[column], mid_columns.at[w, here],
                                col_send.at[w, a * 2 + q], col_recv.at[w, here], (dest_e, q, t),
                            )
                        )

    column_copies(lambda copy: copy.start())

    @pl.when(direct_half)
    def _():
        base = lax.rem(e, half_experts) - low
        mid_columns[0, here] = mid_stage[(base + low) * 2 + p]
        mid_columns[1, here] = mid_stage[(base + 1 - low) * 2 + p]

    lane_causal = row[:BLK, :BLK] >= col[:BLK, :BLK]
    lane_causal_t = row[:BLK, :BLK] <= col[:BLK, :BLK]
    for n in range(blocks - 1, -1, -1):
        for h in range(heads):
            ks, vs = slice(h * DK, (h + 1) * DK), slice(h * DV, (h + 1) * DV)
            o, v = o_all[span[n], vs], v_all[span[n], vs]
            qg, kk = q_grow[n][:, ks], k_shrink[n][:, ks]
            state_in = block_states[n, h].astype(bf16)
            scores = jnp.where(lane_causal, dot(o, v, ACROSS), 0.0)
            scores_t = jnp.where(lane_causal_t, dot(v, o, ACROSS), 0.0)
            mutual_t = jnp.where(lane_causal_t, dot(kk, qg, ACROSS), 0.0)
            gq = growth[n][:, ks] * (dot(o, state_in, ACROSS) + dot(scores, kk))
            gk = shrink[n][:, ks] * dot(scores_t, qg)
            gv = dot(mutual_t, o)
            if n < blocks - 1:
                later = slice((n + 1) * BLK, tokens)
                end = position[(n + 1) * BLK - 1 : (n + 1) * BLK, ks]
                carried = dot(
                    q_all[later, ks] * jnp.exp(position[later, ks] - end), o_all[later, vs], DOWNWARD
                )
                gk = gk + to_end[n][:, ks] * dot(v, carried, ACROSS)
                gv = gv + dot(k_end[n][:, ks], carried)
            grad_q[span[n], ks] = gq
            key_local[span[n], ks] = gk
            value_local[span[n], vs] = gv
    contrib = q_all * grad_q[...] - k_all * key_local[...]
    contrib_local[...] = contrib
    gathered[me] = jnp.sum(contrib, axis=0, keepdims=True)
    for k in range(1, count):
        spread(lambda i: gathered.at[me], gathered.at[me], term_send, term_recv, k).start()

    lax.fori_loop(first_cut, second_cut, weight_step, 0)
    for k in range(1, count):
        landed(early_held, early_send, early_recv, k)
        landed(sum_held, sum_send, sum_recv, k)
        landed(gains, gain_send, gain_recv, k)
    total = jnp.zeros((rows, DV), f32)
    dots = jnp.zeros((rows, 1), f32)
    table = jnp.zeros((rows, 128), f32)
    table_lane = lax.broadcasted_iota(jnp.int32, (rows, 128), 1)
    table_row = lax.broadcasted_iota(jnp.int32, (rows, 128), 0)
    channel = lax.broadcasted_iota(jnp.int32, (rows, channels), 1)
    owned = channel == me * rows + lax.broadcasted_iota(jnp.int32, (rows, channels), 0)
    for i in range(count - 1, -1, -1):
        result[i] = total.astype(bf16)
        table = jnp.where(table_lane == i, dots, table)
        dots = dots + jnp.sum(early_held[i].astype(f32) * total, axis=1, keepdims=True)
        gain = jnp.sum(jnp.where(owned, gains[i], 0.0), axis=1, keepdims=True)
        total = gain * total + sum_held[i].astype(f32)
    spread_out = (table_lane == lax.rem(me * rows, 128) + table_row).astype(f32)
    turned = lax.dot_general(
        table, spread_out, DOWNWARD, precision=PRECISE, preferred_element_type=f32
    )
    for i in range(count):
        dot_result[i] = turned[i : i + 1]
    from_right[me] = result[me]
    decay_dots[me] = dot_result[me]
    def right_copy(k):
        return spread(lambda i: result.at[i], from_right.at[me], right_send, right_recv, k)

    def dot_copy(k):
        return spread(lambda i: dot_result.at[i], decay_dots.at[me], dot_send, dot_recv, k)

    for k in range(1, count):
        right_copy(k).start()
        dot_copy(k).start()

    def cross_copy():
        return remote(mid_columns, mid_columns, cross_send, cross_recv, mate_id)

    @pl.when(direct_half)
    def _():
        for k in range(1, share):
            source = lax.rem(here + k, share)
            for w in range(2):
                spot = mid_columns.at[w, source]
                remote(
                    spot, spot, col_send.at[w, 0], col_recv.at[w, source], mate_id
                ).wait_recv()
        cross_copy().start()

    lax.fori_loop(second_cut, weight_steps, weight_step, 0)

    @pl.when(jnp.logical_not(direct_half))
    def _():
        cross_copy().wait_recv()

    for k in range(half_experts):
        mixer_side(k, 1 - p).wait_recv()
    for w in (1, 0):
        product = dot(
            mid_columns[w].reshape(share * tokens, piece),
            mixers[...].reshape(share * tokens, mixers.shape[2]),
            DOWNWARD,
        )
        if w:
            near_part[...] = product
            near = remote(near_part, near_held, near_send, near_recv, (flip(1), p, t))
            near.start()
        else:
            grad_out[...] = product
    near.wait_recv()
    grad_out[...] = grad_out[...] + near_held[...]
    for k in range(1, count):
        landed(gathered, term_send, term_recv, k)
    summed_terms = jnp.zeros((1, channels), f32)
    for i in range(count):
        summed_terms += jnp.where(i > me, gathered[i], 0.0)
    right_terms[...] = summed_terms
    for k in range(1, count):
        landed(from_right, right_send, right_recv, k)
        landed(decay_dots, dot_send, dot_recv, k)
    to_core(own_columns).wait_send()
    near.wait_send()
    column_copies(lambda copy: copy.wait_send())

    @pl.when(direct_half)
    def _():
        cross_copy().wait_send()

    for k in range(1, count):
        early_copy(k).wait_send()
        gain_copy(k).wait_send()
        spread(lambda i: sum_stage.at[i], sum_held.at[me], sum_send, sum_recv, k).wait_send()
        right_copy(k).wait_send()
        dot_copy(k).wait_send()
        spread(lambda i: gathered.at[me], gathered.at[me], term_send, term_recv, k).wait_send()

    def close(k, carry):
        for a in range(2):
            to_pair(a, k, p).wait_send()
            to_mate(a, k, p, 0, own_columns).wait_send()
            to_mate(a, k, 1 - p, 1, own_columns).wait_send()
        core_copy(0, k).wait_send()
        core_copy(1, k).wait_send()
        pair_copy(k).wait_send()

        @pl.when(k > 0)
        def _():
            direct(0, k).wait_send()
            direct(1, k).wait_send()
            back_copy(k).wait_send()

        return carry

    lax.fori_loop(0, experts, close, 0)
    for k in range(half_experts):
        if k:
            mixer_copy(k).wait_send()
        mixer_side(k, p).wait_send()


def layer_back(
    cap, ids, route_weights, moe_input, out_grad, gate_w, up_w, down_w, mixer, out_weight,
    queries, keys, values, log_decay, block_states,
):
    experts = lax.axis_size("ep")
    count = experts * 2
    tokens, model_width = moe_input.shape
    units = gate_w.shape[1]
    width = model_width // lax.axis_size("tp")
    slots = experts * 2 * cap
    channels = queries.shape[1]
    rows = channels // count
    share = count // 2
    piece = width // share
    half = (experts, cap, width)
    vmem = pl.BlockSpec(memory_space=pltpu.VMEM)
    hbm = pl.BlockSpec(memory_space=pltpu.HBM)
    dma = pltpu.SemaphoreType.DMA
    wide, tall = (model_width, units), (units, model_width)
    kind, f32 = jnp.bfloat16, jnp.float32
    shape = jax.ShapeDtypeStruct
    group_rows = PER_GROUP * 2 * cap
    local = shape((tokens, channels), f32)
    keep = pltpu.VMEM
    grant = 40 if slots * model_width <= 3 << 19 else 60
    return pl.pallas_call(
        functools.partial(experts_kernel, experts, cap),
        out_shape=(
            shape(wide, kind),
            shape(wide, kind),
            shape(tall, kind),
            shape((piece, mixer.shape[1]), f32),
            shape((count, rows, DV), kind),
            shape((count, 1, 128), f32),
            shape((1, channels), f32),
            local,
            local,
            shape(values.shape, f32),
            local,
            local,
            local,
        ),
        in_specs=[vmem] * 4 + [hbm] * 10,
        out_specs=(vmem,) * 13,
        scratch_shapes=[
            keep(out_weight.shape, kind),
            keep(queries.shape, kind),
            keep(keys.shape, kind),
            keep(values.shape, kind),
            keep(log_decay.shape, f32),
            keep(block_states.shape, f32),
            keep((share,) + mixer.shape, kind),
            keep((experts * cap, width), kind),
            keep((tokens, channels), f32),
            keep((tokens, model_width), kind),
            keep((share, tokens, piece), kind),
            keep((2, share, tokens, piece), kind),
            keep((count, rows, DV), kind),
            keep((count, rows, DV), kind),
            keep((count, rows, DV), kind),
            keep((count, rows, DV), kind),
            keep((count, rows, DV), kind),
            keep((count, 1, 128), f32),
            keep((count, 1, channels), f32),
            keep((count, 1, channels), f32),
            keep((piece, mixer.shape[1]), f32),
            keep((piece, mixer.shape[1]), f32),
            keep((slots, model_width), kind),
            keep((slots, model_width), kind),
            keep((slots, units), kind),
            keep((slots, 2 * units), kind),
            keep((model_width, 2 * units), kind),
            keep(tall, kind),
            keep((group_rows, units), f32),
            keep((group_rows, units), f32),
            keep((slots, model_width), kind),
            keep((experts, tokens), jnp.int32),
            keep(half, kind),
            keep(half, kind),
            keep((2,) + half, kind),
            keep(half, kind),
            dma((3,)),
            *(dma((2, experts)) for _ in range(4)),
            *(dma((2, 2, experts)) for _ in range(2)),
            *(dma((2, experts)) for _ in range(2)),
            *(dma((experts,)) for _ in range(4)),
            dma((7,)),
            *(dma((experts // 2,)) for _ in range(4)),
            dma,
            dma,
            dma((2, share)),
            dma((2, share)),
            *(dma for _ in range(4)),
            *(dma((count,)) for _ in range(12)),
        ],
        compiler_params=pltpu.CompilerParams(
            collective_id=0, has_side_effects=True, vmem_limit_bytes=grant * 1024 * 1024
        ),
        name="layer_back",
    )(
        *(
            pltpu.with_memory_space_constraint(x, pltpu.HBM)
            for x in (
                ids, route_weights, moe_input, out_grad, gate_w, up_w, down_w, mixer, out_weight,
                queries, keys, values, log_decay, block_states,
            )
        )
    )


def finish_kernel(
    chunks, weight_a, weight_b, weight_c, *refs,
):
    f32, bf16 = jnp.float32, jnp.bfloat16
    sources, targets, holds = refs[:11], refs[11:19], refs[19:30]
    small_sem, out_sem = refs[30:]
    grad_q, grad_k, grad_v, grad_decay, grad_out, out_a, out_b, out_c = targets
    pairs = ((weight_a, out_a), (weight_b, out_b), (weight_c, out_c))
    small = [
        pltpu.make_async_copy(src, dst, small_sem.at[i])
        for i, (src, dst) in enumerate(zip(sources, holds))
    ]

    def move(a, j):
        source, target = pairs[a]
        size = source.shape[0] // chunks
        cut = pl.ds(j * size, size)
        return pltpu.make_async_copy(source.at[cut], target.at[cut], out_sem.at[a, j])

    steps = [(a, j) for a in range(3) for j in range(chunks)]
    for copy in small:
        copy.start()
    for a, j in steps:
        move(a, j).start()

    def dot(x, y, dims=PLAIN):
        return lax.dot_general(
            x.astype(bf16), y.astype(bf16), dims, preferred_element_type=f32
        )

    for copy in small:
        copy.wait()
    (
        grad_out_turned, from_right, decay_dots, right_terms, query_local, key_local, value_local,
        contrib_local, k_fade, fade_out, values,
    ) = holds
    tokens, channels = key_local.shape
    heads = channels // DK
    grad_q[...] = query_local[...].astype(bf16)
    key_parts = []
    for h in range(heads):
        ks, vs = slice(h * DK, (h + 1) * DK), slice(h * DV, (h + 1) * DV)
        carried = from_right[h]
        key_parts.append(dot(values[:, vs], carried, ACROSS))
        grad_v[:, vs] = (value_local[:, vs] + dot(k_fade[:, ks], carried)).astype(bf16)
    key_part = jnp.concatenate(key_parts, axis=1)
    grad_k[...] = (key_local[...] + fade_out[...] * key_part).astype(bf16)
    contrib = contrib_local[...] - k_fade[...] * key_part
    row = lax.broadcasted_iota(jnp.int32, (tokens, tokens), 0)
    col = lax.broadcasted_iota(jnp.int32, (tokens, tokens), 1)
    later = (col >= row).astype(f32)
    owners = decay_dots.shape[0]
    each = owners * 128 // channels
    groups = [
        jnp.sum(decay_dots[g * each : (g + 1) * each, 0], axis=0, keepdims=True)
        for g in range(channels // 128)
    ]
    right = right_terms[...] - jnp.concatenate(groups, axis=1)
    grad_decay[...] = right + lax.dot_general(
        later, contrib, PLAIN, precision=PRECISE, preferred_element_type=f32
    )
    grad_out[...] = jnp.transpose(grad_out_turned[...])
    for a, j in steps:
        move(a, j).wait()


def finish(local, values, weights):
    grad_out_turned, from_right, decay_dots, right_terms, *rest = local
    tokens, channels = rest[1].shape
    heads = channels // DK
    from_right = from_right.reshape(heads, DK, DV)
    vmem = pl.BlockSpec(memory_space=pltpu.VMEM)
    hbm = pl.BlockSpec(memory_space=pltpu.HBM)
    dma = pltpu.SemaphoreType.DMA
    shape = jax.ShapeDtypeStruct
    f32, bf16 = jnp.float32, jnp.bfloat16
    chunks = 8
    smalls = (
        grad_out_turned, from_right, decay_dots, right_terms, *rest, values,
    )
    return pl.pallas_call(
        functools.partial(finish_kernel, chunks),
        out_shape=(
            shape((tokens, channels), bf16),
            shape((tokens, channels), bf16),
            shape((tokens, heads * DV), bf16),
            shape((tokens, channels), f32),
            shape(grad_out_turned.shape[::-1], f32),
            *(shape(w.shape, w.dtype) for w in weights),
        ),
        in_specs=[vmem] * 3 + [hbm] * 11,
        out_specs=(vmem,) * 5 + (hbm,) * 3,
        scratch_shapes=[pltpu.VMEM(w.shape, w.dtype) for w in smalls]
        + [dma((11,)), dma((3, chunks))],
        compiler_params=pltpu.CompilerParams(vmem_limit_bytes=8 * 1024 * 1024),
        name="finish",
    )(*weights, *smalls)


def body(
    moe_input,
    out_grad,
    route_ids,
    route_weights,
    gate_w,
    up_w,
    down_w,
    mixer_out,
    out_weight,
    queries,
    keys,
    values,
    log_decay,
    block_states,
):
    experts = lax.axis_size("ep")
    cap = -(-3 * moe_input.shape[0] // experts // 16) * 16
    results = layer_back(
        cap, route_ids.T, route_weights.T, moe_input, out_grad, gate_w[0], up_w[0], down_w[0],
        mixer_out, out_weight, queries, keys, values, log_decay, block_states,
    )
    weights, local = results[:3], results[3:]
    grad_q, grad_k, grad_v, grad_decay, grad_out_weight, grad_gate, grad_up, grad_down = finish(
        local, values, weights
    )
    return (
        grad_q,
        grad_k,
        grad_v,
        grad_decay,
        grad_out_weight,
        grad_gate[None],
        grad_up[None],
        grad_down[None],
    )


def solution(mesh):
    sp_count, tp_count = mesh.devices.shape
    mesh = Mesh(mesh.devices.reshape(sp_count // 2, 2, tp_count), ("ep", "pair", "tp"))
    placed = (
        P(SP, None),
        P(SP, None),
        P(SP, None),
        P(SP, None),
        P(SP, None, "tp"),
        P(SP, None, "tp"),
        P(SP, "tp", None),
        P(SP, "tp"),
        P("tp", None),
        P(SP, "tp"),
        P(SP, "tp"),
        P(SP, "tp"),
        P(SP, "tp"),
        P(SP, "tp", None, None),
    )
    return jax.shard_map(
        body,
        mesh=mesh,
        in_specs=placed,
        out_specs=(
            P(SP, "tp"),
            P(SP, "tp"),
            P(SP, "tp"),
            P(SP, "tp"),
            P("tp", SP),
            P(SP, None, "tp"),
            P(SP, None, "tp"),
            P(SP, "tp", None),
        ),
        check_vma=False,
    )
```
